512 devices in a mesh: ep: 32 (over z, core), tp: 16 (over y, x).
Axes of the slice: x: 4, y: 4, z: 16, core: 2. Of those that a mesh axis runs over, the one named last changes fastest.
Arguments:
- queries: bfloat16 [8192, 2048], P('ep', 'tp'), may hold values from -6 to 6
- keys: bfloat16 [8192, 2048], P('ep', 'tp'), may hold values from -6 to 6
- values: bfloat16 [8192, 2048], P('ep', 'tp'), may hold values from -6 to 6
- gates: bfloat16 [8192, 2048], P('ep', 'tp'), may hold values from -6 to 6
- log_decay: float32 [8192, 16], P('ep', 'tp'), may hold values from -2 to 0
- out_weight: bfloat16 [2048, 2048], P(None, 'tp'), may hold values from -0.125 to 0.125
- moe_rows: bfloat16 [8192, 2048], P('ep'), may hold values from -140 to 140
- moe_gain: bfloat16 [2048], replicated, may hold values from 0.099609375 to 1.8984375
- routes: int32 [8192, 2], P('ep'), may hold values from 0 to 31, as said below
- route_weights: float32 [8192, 2], P('ep'), may hold values from 0.1 to 1
- gate_proj: bfloat16 [32, 2048, 4096], P('ep', None, 'tp'), may hold values from -0.125 to 0.125
- up_proj: bfloat16 [32, 2048, 4096], P('ep', None, 'tp'), may hold values from -0.125 to 0.125
- down_proj: bfloat16 [32, 4096, 2048], P('ep', None, 'tp'), may hold values from -0.09375 to 0.09375
Outputs:
- mixer_out: bfloat16 [8192, 2048], P('ep', 'tp')
- moe_out: bfloat16 [8192, 2048], P('ep', 'tp')
The draws below stay inside these ranges and needn't reach their ends.
Inputs may be any that keep to these rules, and one draw needn't show every extreme that they name: `routes`: each row names two different experts of one group of 8 consecutive experts; in each aligned block of 256 rows every expert is named by exactly 16 rows.
All inputs are finite; a program needn't handle non-finite values.
Results may differ from the reference program's by a relative error of at most 0.011.
Values may be sent and summed in bfloat16 or wider, within the bound.
No kernel may reach another device: no remote copies, remote signals or barrier semaphores. Data moves between devices by JAX's collectives and lax.ppermute only.
A program may use at most 64 MiB of HBM per device.

```python
import math
import jax
import jax.numpy as jnp
from jax import lax

D = 2048
RETENTION_HEADS = 16
HEAD_DIM = 128
FF = 4096
EXP_GROUP = 8
BLOCK = 128
ROWS_MIX = 256
ROWS_MOE = 256
MIXER_TOKENS = 8192
TOKENS_MOE = 8192
EXPERTS = 32
GROUPS = 4


def draw_log_decay(key, part):
    k_fast = jax.random.fold_in(key, 11)
    k_rate = jax.random.fold_in(key, 12)
    k_slow = jax.random.fold_in(key, 13)
    k_block = jax.random.fold_in(key, 14)
    k_rough = jax.random.fold_in(key, 15)
    location_random_key = jax.random.fold_in(key, 16)
    spike_random_key = jax.random.fold_in(key, 17)
    fast_share = 0.5
    is_fast = jax.random.uniform(k_fast, (RETENTION_HEADS,)) < fast_share
    fast_rate = jax.random.uniform(k_rate, (RETENTION_HEADS,), minval=2.5, maxval=4.0) / BLOCK
    slow_rate = jax.random.uniform(k_slow, (RETENTION_HEADS,), minval=0.1, maxval=0.35) / MIXER_TOKENS
    baseline_decay_rate = jnp.where(is_fast, fast_rate, slow_rate)
    span_count = MIXER_TOKENS // ROWS_MIX
    extent_multiplier = jnp.exp(jax.random.uniform(k_block, (span_count, RETENTION_HEADS), minval=-math.log(2.0), maxval=math.log(2.0)))
    extent_multiplier = jnp.repeat(extent_multiplier, ROWS_MIX, axis=0)
    jitter_multiplier = jnp.exp(jax.random.uniform(k_rough, (MIXER_TOKENS, RETENTION_HEADS), minval=-0.7, maxval=0.7))
    spike_locations = jax.random.randint(location_random_key, (2, RETENTION_HEADS), 0, MIXER_TOKENS)
    spike_strength = jnp.log(jax.random.uniform(spike_random_key, (2, RETENTION_HEADS), minval=0.5, maxval=0.8))
    token_place = jnp.arange(MIXER_TOKENS, dtype=jnp.int32)[None, :, None]
    decay_spikes = jnp.sum(jnp.where(token_place == spike_locations[:, None, :], spike_strength[:, None, :], 0.0), axis=0)
    return (decay_spikes - baseline_decay_rate[None, :] * extent_multiplier * jitter_multiplier).astype(jnp.float32)


def draw_moe_rows(key, part):
    k_base = jax.random.fold_in(key, 21)
    k_column = jax.random.fold_in(key, 22)
    base = jax.random.truncated_normal(k_base, -4.0, 4.0, (TOKENS_MOE, D))
    column_scale = jnp.exp(jax.random.uniform(k_column, (D,), minval=0.0, maxval=math.log(10.0)))
    result = base * column_scale[None, :]
    return result.astype(jnp.bfloat16)


def draw_routes(key, part):
    k_perm = jax.random.fold_in(key, 31)
    k_first = jax.random.fold_in(key, 32)
    k_second = jax.random.fold_in(key, 33)
    span_count = TOKENS_MOE // ROWS_MOE
    orders = jax.vmap(lambda single: jax.random.permutation(single, ROWS_MOE))(jax.random.split(k_perm, span_count))
    ranked = jnp.argsort(orders, axis=1, stable=True).astype(jnp.int32)
    group_id = ranked % GROUPS
    local_rank = ranked // GROUPS
    first_offset = jax.random.randint(k_first, (span_count, GROUPS), 0, EXP_GROUP)
    second_offset = jax.random.randint(k_second, (span_count, GROUPS), 0, EXP_GROUP - 1)
    first_pick = (local_rank + jnp.take_along_axis(first_offset, group_id, axis=1)) % EXP_GROUP
    second_step = (local_rank // EXP_GROUP + jnp.take_along_axis(second_offset, group_id, axis=1)) % (EXP_GROUP - 1)
    second_pick = (first_pick + 1 + second_step) % EXP_GROUP
    chosen = jnp.stack([group_id * EXP_GROUP + first_pick, group_id * EXP_GROUP + second_pick], axis=-1)
    return chosen.reshape(TOKENS_MOE, 2).astype(jnp.int32)


def block_levels(stream_key, dims, cuts, least, high):
    def one(dim, shards_of):
        draws = jax.random.uniform(jax.random.fold_in(jax.random.fold_in(stream_key, 6), dim), (shards_of,), jnp.float32, least / len(cuts), high / len(cuts))
        return jnp.repeat(jnp.exp(draws), dims[dim] // shards_of).reshape((-1,) + (1,) * (len(dims) - dim - 1))

    gain = one(*cuts[0])
    for cut in cuts[1:]:
        gain = gain * one(*cut)
    return gain


def centred(own_key, extent, scale, limit, cuts=(), kind=jnp.bfloat16):
    level = block_levels(own_key, extent, cuts, -0.22, 0.18) if cuts else 1.0
    drawn = jax.random.normal(own_key, extent, jnp.float32) * scale * level
    return jnp.minimum(jnp.maximum(drawn, -limit), limit).astype(kind)


def setup_inputs(seed: int = 0) -> dict:
    arg_keys = jax.random.split(jax.random.key(seed), 14)
    queries = centred(arg_keys[0], (MIXER_TOKENS, RETENTION_HEADS * HEAD_DIM), 1.0, 6.0, ((0, 32), (1, 16)))
    keys = centred(arg_keys[1], (MIXER_TOKENS, RETENTION_HEADS * HEAD_DIM), 1.0, 6.0, ((0, 32), (1, 16)))
    values = centred(arg_keys[2], (MIXER_TOKENS, RETENTION_HEADS * HEAD_DIM), 1.0, 6.0, ((0, 32), (1, 16)))
    gates = centred(arg_keys[3], (MIXER_TOKENS, RETENTION_HEADS * HEAD_DIM), 1.0, 6.0, ((0, 32), (1, 16)))
    log_decay = draw_log_decay(jax.random.fold_in(arg_keys[13], 71), 0)
    out_weight = centred(arg_keys[5], (RETENTION_HEADS * HEAD_DIM, D), (RETENTION_HEADS * HEAD_DIM) ** -0.5, 0.125, ((1, 16),))
    moe_rows = draw_moe_rows(jax.random.fold_in(arg_keys[13], 71), 0)
    moe_gain = jnp.clip(1.0 + 0.18 * jax.random.normal(arg_keys[7], (D,), jnp.float32), 0.099609375, 1.8984375).astype(jnp.bfloat16)
    routes = draw_routes(jax.random.fold_in(arg_keys[13], 71), 0)
    route_weights = jnp.clip(0.1 + 0.9 * jax.random.uniform(arg_keys[9], (TOKENS_MOE, 2), jnp.float32) ** block_levels(arg_keys[9], (TOKENS_MOE, 2), ((0, 32),), -0.2, 0.2), 0.1, 1.0)
    gate_proj = centred(arg_keys[10], (EXPERTS, D, FF), D ** -0.5, 0.125, ((0, 32), (2, 16)))
    up_proj = centred(arg_keys[11], (EXPERTS, D, FF), D ** -0.5, 0.125, ((0, 32), (2, 16)))
    down_proj = centred(arg_keys[12], (EXPERTS, FF, D), FF ** -0.5, 0.09375, ((0, 32), (2, 16)))
    return {"queries": queries, "keys": keys, "values": values, "gates": gates, "log_decay": log_decay, "out_weight": out_weight, "moe_rows": moe_rows, "moe_gain": moe_gain, "routes": routes, "route_weights": route_weights, "gate_proj": gate_proj, "up_proj": up_proj, "down_proj": down_proj}


def rotate(source, factor):
    length = source.shape[0]
    values_f = source.astype(jnp.float32).reshape(length, RETENTION_HEADS, HEAD_DIM)
    half_dim = HEAD_DIM // 2
    inverse = 10000.0 ** (-jnp.arange(half_dim, dtype=jnp.float32) / half_dim)
    angles = jnp.arange(length, dtype=jnp.float32)[:, None] * inverse[None, :]
    cosine = jnp.cos(angles)[:, None, :]
    sine_part = jnp.sin(angles)[:, None, :]
    first_half = values_f[..., :half_dim]
    second_half = values_f[..., half_dim:]
    turned = jnp.concatenate([first_half * cosine - second_half * sine_part, first_half * sine_part + second_half * cosine], axis=-1)
    return (turned * factor).astype(jnp.bfloat16)

def retention_ref(queries, keys, values, gates, log_decay, out_weight):
    length = queries.shape[0]
    block_count = length // BLOCK
    rot_q = rotate(queries, 1.0)
    rot_k = rotate(keys, HEAD_DIM ** (-0.5))
    q_blocks = rot_q.reshape(block_count, BLOCK, RETENTION_HEADS, HEAD_DIM)
    k_blocks = rot_k.reshape(block_count, BLOCK, RETENTION_HEADS, HEAD_DIM)
    v_blocks = values.reshape(block_count, BLOCK, RETENTION_HEADS, HEAD_DIM)
    l_blocks = log_decay.reshape(block_count, BLOCK, RETENTION_HEADS)
    causal = jnp.arange(BLOCK)[:, None] >= jnp.arange(BLOCK)[None, :]

    def advance(carry_state, member):
        q_block, k_block, v_block, l_block = member
        cumulative = jnp.cumsum(l_block, axis=0)
        across = cumulative.T
        spread = across[:, :, None] - across[:, None, :]
        weights = jnp.where(causal, jnp.exp(jnp.where(causal, spread, 0.0)), 0.0)
        q_float = q_block.astype(jnp.float32)
        k_float = k_block.astype(jnp.float32)
        v_float = v_block.astype(jnp.float32)
        scores = jnp.einsum('ihd,jhd->hij', q_float, k_float)
        rounded = lax.optimization_barrier((scores * weights).astype(jnp.bfloat16)).astype(jnp.float32)
        inside = jnp.einsum('hij,jhd->ihd', rounded, v_float)
        carried = jnp.einsum('ihd,hde->ihe', q_float, carry_state, precision=lax.Precision.HIGHEST) * jnp.exp(cumulative)[:, :, None]
        ending = cumulative[-1]
        k_scaled = k_float * jnp.exp(ending[None, :] - cumulative)[:, :, None]
        update = jnp.einsum('jhd,jhe->hde', k_scaled, v_float, precision=lax.Precision.HIGHEST)
        return (jnp.exp(ending)[:, None, None] * carry_state + update, inside + carried)
    zero_state = jnp.zeros((RETENTION_HEADS, HEAD_DIM, HEAD_DIM), jnp.float32)
    _, retained = lax.scan(advance, zero_state, (q_blocks, k_blocks, v_blocks, l_blocks))
    retained = retained.reshape(length, RETENTION_HEADS, HEAD_DIM)
    gate_f = gates.astype(jnp.float32).reshape(length, RETENTION_HEADS, HEAD_DIM)
    scaled = retained * lax.rsqrt(lax.optimization_barrier(jnp.mean(retained * retained, axis=-1, keepdims=True)) + 1e-05)
    head_out = (scaled * jax.nn.silu(gate_f)).astype(jnp.bfloat16).reshape(length, RETENTION_HEADS * HEAD_DIM)
    return jnp.dot(head_out, out_weight, preferred_element_type=jnp.float32).astype(jnp.bfloat16)

def experts_ref(moe_rows, moe_gain, routes, route_weights, gate_proj, up_proj, down_proj):
    as_float = moe_rows.astype(jnp.float32)
    normed = (as_float * lax.rsqrt(lax.optimization_barrier(jnp.mean(as_float * as_float, axis=-1, keepdims=True)) + 1e-06) * moe_gain.astype(jnp.float32)).astype(jnp.bfloat16)
    flat_ids = routes.reshape(-1)
    sorted_slots = jnp.argsort(flat_ids, stable=True).astype(jnp.int32)
    per_expert = flat_ids.shape[0] // EXPERTS
    grouped = normed[sorted_slots // 2].reshape(EXPERTS, per_expert, D)

    def run_expert(member):
        block_rows, w_gate, w_up, w_down = member
        gate_part = jnp.dot(block_rows, w_gate, preferred_element_type=jnp.float32)
        up_part = jnp.dot(block_rows, w_up, preferred_element_type=jnp.float32)
        hidden = (jax.nn.silu(gate_part) * up_part).astype(jnp.bfloat16)
        return jnp.dot(hidden, w_down, preferred_element_type=jnp.float32).astype(jnp.bfloat16)
    outputs = lax.map(run_expert, (grouped, gate_proj, up_proj, down_proj))
    slot_out = jnp.zeros((flat_ids.shape[0], D), jnp.bfloat16).at[sorted_slots].set(outputs.reshape(-1, D))
    weighted = slot_out.astype(jnp.float32).reshape(-1, 2, D) * route_weights[:, :, None]
    return lax.optimization_barrier(jnp.sum(weighted, axis=1)).astype(jnp.bfloat16)

def reference(queries, keys, values, gates, log_decay, out_weight, moe_rows, moe_gain, routes, route_weights, gate_proj, up_proj, down_proj):
    mixer_out = retention_ref(queries, keys, values, gates, log_decay, out_weight)
    moe_out = experts_ref(moe_rows, moe_gain, routes, route_weights, gate_proj, up_proj, down_proj)
    return (mixer_out, moe_out)
```

```python
import jax
import jax.numpy as jnp
from jax import lax
from jax.experimental import pallas as pl
from jax.experimental.pallas import tpu as pltpu
from jax.sharding import Mesh
from jax.sharding import PartitionSpec as P

BLOCK = 128
HEAD = 128
EP = ("ep_0", "ep_1")
TP = ("tp_0", "tp_1")
BF = jnp.bfloat16
F32 = jnp.float32
HIGH = lax.Precision.HIGHEST
PAY = HEAD + 16


def dot(a, b, dims=((1,), (0,)), precision=None):
    return lax.dot_general(a, b, (dims, ((), ())), precision=precision, preferred_element_type=F32)


def call(body, out_shape, *args, name):
    return pl.pallas_call(body, out_shape=out_shape, name=name)(*args)


def shaped(shape, dtype):
    return jax.ShapeDtypeStruct(shape, dtype)


def route_body(turn, routes, rows, part, gain, send, slots):
    tokens = rows.shape[0]
    experts = send.shape[0]
    room = send.shape[1]
    wide = rows[...].astype(F32)
    power = jnp.mean(wide * wide, axis=-1, keepdims=True)
    normed = (part[...].astype(F32) * lax.rsqrt(power + 1e-06) * gain[...].astype(F32)).astype(BF)
    first = routes[0:1, :]
    second = routes[1:2, :]
    expert = lax.broadcasted_iota(jnp.int32, (experts, tokens), 0)
    is_first = expert == first
    is_second = expert == second
    named = jnp.where(is_first | is_second, 1.0, 0.0).astype(BF)
    earlier = lax.broadcasted_iota(jnp.int32, (tokens, tokens), 0) < lax.broadcasted_iota(
        jnp.int32, (tokens, tokens), 1
    )
    rank = dot(named, jnp.where(earlier, 1.0, 0.0).astype(BF)).astype(jnp.int32)
    slot_a = first * room + jnp.sum(jnp.where(is_first, rank, 0), axis=0, keepdims=True)
    slot_b = second * room + jnp.sum(jnp.where(is_second, rank, 0), axis=0, keepdims=True)
    slots[0:1, :] = slot_a
    slots[1:2, :] = slot_b
    place = lax.broadcasted_iota(jnp.int32, (experts * room, tokens), 0)
    chosen = jnp.where((place == slot_a) | (place == slot_b), 1.0, 0.0).astype(BF)
    send[...] = dot(chosen, normed).astype(BF).reshape(experts, room, HEAD)


def dispatch(moe_rows, moe_gain, routes, experts, turn):
    tokens, width = moe_rows.shape
    room = 2 * tokens // experts
    grid = pltpu.PrefetchScalarGridSpec(
        num_scalar_prefetch=1,
        grid=(1,),
        in_specs=[
            pl.BlockSpec((2, tokens), lambda i, t: (0, 0)),
            pl.BlockSpec((tokens, width), lambda i, t: (0, 0)),
            pl.BlockSpec((tokens, HEAD), lambda i, t: (0, t[0])),
            pl.BlockSpec((1, HEAD), lambda i, t: (0, t[0])),
        ],
        out_specs=[
            pl.BlockSpec((experts, room, HEAD), lambda i, t: (0, 0, 0)),
            pl.BlockSpec((2, tokens), lambda i, t: (0, 0)),
        ],
    )
    return pl.pallas_call(
        route_body,
        grid_spec=grid,
        out_shape=[shaped((experts, room, HEAD), BF), shaped((2, tokens), jnp.int32)],
        name="route",
    )(turn, routes.T, moe_rows, moe_rows, moe_gain.reshape(1, width))


def hidden_body(rows, w_gate, w_up, head_out, out, acc_gate, acc_up):
    step = pl.program_id(0)

    @pl.when(step == 0)
    def _():
        acc_gate[...] = jnp.zeros_like(acc_gate)
        acc_up[...] = jnp.zeros_like(acc_up)

    left = jnp.concatenate([rows[k] for k in range(rows.shape[0])], axis=1)
    acc_gate[...] += dot(left, w_gate[0])
    acc_up[...] += dot(left, w_up[0])

    @pl.when(step == pl.num_programs(0) - 1)
    def _():
        gate = acc_gate[...]
        hidden = (gate / (1.0 + jnp.exp(-gate)) * acc_up[...]).astype(BF)
        count = hidden.shape[0]
        for k in range(out.shape[0]):
            out[k, 0:count, :] = hidden[:, 0:HEAD]
            out[k, count : 2 * count, :] = hidden[:, HEAD:]
            out[k, 2 * count :, :] = head_out[...]


def hidden_stage(rows, w_gate, w_up, head_out, copies):
    parts, count, _ = rows.shape
    units = w_gate.shape[2]
    per = 4
    steps = parts // per
    tall = 2 * count + head_out.shape[0]
    return pl.pallas_call(
        hidden_body,
        grid=(steps,),
        in_specs=[
            pl.BlockSpec((per, count, HEAD), lambda i: (i, 0, 0)),
            pl.BlockSpec((1, per * HEAD, units), lambda i: (0, i, 0)),
            pl.BlockSpec((1, per * HEAD, units), lambda i: (0, i, 0)),
            pl.BlockSpec(head_out.shape, lambda i: (0, 0)),
        ],
        out_specs=pl.BlockSpec((copies, tall, HEAD), lambda i: (0, 0, 0)),
        out_shape=shaped((copies, tall, HEAD), BF),
        scratch_shapes=[pltpu.VMEM((count, units), F32), pltpu.VMEM((count, units), F32)],
        name="hidden",
    )(rows, w_gate, w_up, head_out)


def project_body(lane, got, w_0, w_1, w_2, w_3, out):
    peers = got.shape[0]
    count = got.shape[1] * 2 // 5
    positions = got.shape[1] - 2 * count
    units = 2 * HEAD
    left = [
        jnp.concatenate([got[k, 0:count, :], got[k, count : 2 * count, :]], axis=1)
        for k in range(peers)
    ]
    heads = [got[k, 2 * count :, :] for k in range(peers)]
    for first, (one, two) in ((0, (w_0, w_1)), (2, (w_2, w_3))):
        expert = jnp.zeros((count, 2 * HEAD), F32)
        mixer = jnp.zeros((positions, 2 * HEAD), F32)
        for k in range(peers):
            both = jnp.concatenate([one[k], two[k]], axis=1)
            expert += dot(left[k], both[0:units])
            mixer += dot(heads[k], both[units:])
        for which in range(2):
            at = (lane[0] + peers - first - which) % peers
            cols = slice(which * HEAD, which * HEAD + HEAD)
            out[pl.ds(at, 1), 0:count, :] = expert[:, cols].astype(BF)[None]
            out[pl.ds(at, 1), count:, :] = mixer[:, cols].astype(BF)[None]


def project_stage(lane, got, weights):
    peers, tall, _ = got.shape
    count = tall * 2 // 5
    short = count + tall - 2 * count
    return pl.pallas_call(
        project_body,
        in_specs=[pl.BlockSpec(memory_space=pltpu.SMEM)] + [pl.BlockSpec()] * 5,
        out_shape=shaped((peers, short, HEAD), BF),
        name="project",
    )(lane, got, *weights)


def combine_body(back, slots, weights, out):
    experts, room, _ = back.shape
    rows = back[...].reshape(experts * room, HEAD)
    tokens = slots.shape[0]
    place = lax.broadcasted_iota(jnp.int32, (tokens, experts * room), 1)
    total = jnp.zeros((tokens, HEAD), F32)
    for k in range(2):
        chosen = jnp.where(place == slots[:, k : k + 1], 1.0, 0.0).astype(BF)
        total += dot(chosen, rows) * weights[:, k : k + 1]
    out[...] = total.astype(BF)


def local_body(q, k, v, decay, cosine, sine, base, q_decayed, state, pay):
    count = q.shape[0]
    blocks = count // BLOCK
    cos = cosine[...]
    sin = sine[...]
    rows = lax.broadcasted_iota(jnp.int32, (BLOCK, BLOCK), 0)
    cols = lax.broadcasted_iota(jnp.int32, (BLOCK, BLOCK), 1)
    causal = rows >= cols
    upper = jnp.where(rows <= cols, 1.0, 0.0)
    lower = jnp.where(causal, 1.0, 0.0)

    def turned(x, factor):
        wide = x.astype(F32)
        swapped = pltpu.roll(wide, HEAD // 2, 1)
        return ((wide * cos + swapped * sin) * factor).astype(BF)

    q_all = turned(q[...], 1.0)
    k_all = turned(k[...], HEAD ** (-0.5))
    carried = jnp.zeros((HEAD, HEAD), F32)
    leading = jnp.zeros((1, HEAD), F32)
    for n in range(blocks):
        span = slice(n * BLOCK, n * BLOCK + BLOCK)
        q_b, k_b, v_b = q_all[span], k_all[span], v[span, :]
        here = jnp.broadcast_to(decay[n : n + 1, :], (BLOCK, BLOCK))
        cum_i = dot(lower, here, ((1,), (1,)), HIGH)
        cum_j = dot(here, upper, precision=HIGH)
        weights = jnp.where(causal, jnp.exp(jnp.where(causal, cum_i - cum_j, 0.0)), 0.0)
        scores = dot(q_b, k_b, ((1,), (1,)))
        inside = dot((scores * weights).astype(BF), v_b)
        q_f = q_b.astype(F32)
        q_d = q_f * jnp.exp(cum_i)
        if n:
            inside += dot(q_d, carried, precision=HIGH)
        base[span, :] = inside
        q_decayed[span, :] = q_f * jnp.exp(cum_i + leading)
        ending = cum_i[BLOCK - 1 : BLOCK, :]
        k_scaled = k_b.astype(F32) * jnp.exp(ending - cum_i)
        update = dot(k_scaled, v_b.astype(F32), ((0,), (0,)), HIGH)
        carried = jnp.exp(ending) * carried + update
        leading = leading + ending
    state[0:HEAD, :] = carried
    state[HEAD:, :] = jnp.broadcast_to(leading, (8, HEAD))
    packed(pay, carried, leading)


def packed(pay, state, total):
    pay[0:HEAD, :] = state.astype(BF)
    high = total.astype(BF)
    rest = total - high.astype(F32)
    middle = rest.astype(BF)
    low = (rest - middle.astype(F32)).astype(BF)
    row = lax.broadcasted_iota(jnp.int32, (16, HEAD), 0)
    three = jnp.where(
        row == 0,
        high.astype(F32),
        jnp.where(row == 1, middle.astype(F32), jnp.where(row == 2, low.astype(F32), 0.0)),
    )
    pay[HEAD:, :] = three.astype(BF)


def unpacked(pay):
    tail = pay[HEAD:, :].astype(F32)
    return pay[0:HEAD, :].astype(F32), tail[0:1] + tail[1:2] + tail[2:3]


def pair_body(core, own, other, total, pay):
    state, decay = own[0:HEAD, :], own[HEAD : HEAD + 1, :]
    state_o, decay_o = unpacked(other)
    second = core[0] == 1
    early = jnp.where(second, state_o, state)
    late = jnp.where(second, state, state_o)
    late_decay = jnp.where(second, decay, decay_o)
    joined = late + jnp.exp(late_decay) * early
    whole = decay + decay_o
    total[0:HEAD, :] = joined
    total[HEAD:, :] = jnp.broadcast_to(whole, (8, HEAD))
    packed(pay, joined, whole)


def chain_body(before, total, got, before_out, total_out, pay):
    state, decay = unpacked(got)
    behind, behind_decay = before[0:HEAD, :], before[HEAD : HEAD + 1, :]
    before_out[0:HEAD, :] = behind + jnp.exp(behind_decay) * state
    before_out[HEAD:, :] = jnp.broadcast_to(behind_decay + decay, (8, HEAD))
    mine, mine_decay = total[0:HEAD, :], total[HEAD : HEAD + 1, :]
    joined = mine + jnp.exp(mine_decay) * state
    whole = mine_decay + decay
    total_out[0:HEAD, :] = joined
    total_out[HEAD:, :] = jnp.broadcast_to(whole, (8, HEAD))
    packed(pay, joined, whole)


def start_body(total, got, before_out, total_out, pay):
    state, decay = unpacked(got)
    before_out[0:HEAD, :] = state
    before_out[HEAD:, :] = jnp.broadcast_to(decay, (8, HEAD))
    mine, mine_decay = total[0:HEAD, :], total[HEAD : HEAD + 1, :]
    joined = mine + jnp.exp(mine_decay) * state
    whole = mine_decay + decay
    total_out[0:HEAD, :] = joined
    total_out[HEAD:, :] = jnp.broadcast_to(whole, (8, HEAD))
    packed(pay, joined, whole)


def head_body(core, base, q_decayed, before, got, other, gates, out):
    state, _ = unpacked(got)
    behind, behind_decay = before[0:HEAD, :], before[HEAD : HEAD + 1, :]
    entering = behind + jnp.exp(behind_decay) * state
    state_o, decay_o = unpacked(other)
    entering = jnp.where(core[0] == 1, state_o + jnp.exp(decay_o) * entering, entering)
    retained = base[...] + dot(q_decayed[...], entering, precision=HIGH)
    power = jnp.mean(retained * retained, axis=-1, keepdims=True)
    gate = gates[...].astype(F32)
    out[...] = (retained * lax.rsqrt(power + 1e-05) * (gate / (1.0 + jnp.exp(-gate)))).astype(BF)


def smem(count):
    return [pl.BlockSpec(memory_space=pltpu.SMEM)] + [pl.BlockSpec()] * count


def retention_heads(queries, keys, values, gates, log_decay):
    count = queries.shape[0]
    positions = (lax.axis_index(EP) * count + jnp.arange(count, dtype=jnp.int32)).astype(F32)
    half = HEAD // 2
    inverse = 10000.0 ** (-jnp.arange(half, dtype=F32) / half)
    angles = positions[:, None] * jnp.concatenate([inverse, inverse])[None, :]
    cosine = jnp.cos(angles)
    sine = jnp.sin(angles) * jnp.where(jnp.arange(HEAD) < half, -1.0, 1.0)[None, :]
    carry = shaped((HEAD + 8, HEAD), F32)
    pay_shape = shaped((PAY, HEAD), BF)
    flat = shaped((count, HEAD), F32)
    base, q_decayed, own, pay = call(
        local_body,
        [flat, flat, carry, pay_shape],
        queries,
        keys,
        values,
        log_decay.reshape(count // BLOCK, BLOCK),
        cosine,
        sine,
        name="local",
    )
    core = lax.axis_index("ep_1").reshape(1)
    other = lax.ppermute(pay, "ep_1", [(0, 1), (1, 0)])
    total, pay = pl.pallas_call(
        pair_body, in_specs=smem(2), out_shape=[carry, pay_shape], name="pair"
    )(core, own, other)
    chips = lax.axis_size("ep_0")
    before = None
    reach = 1
    while reach < chips:
        got = lax.ppermute(pay, "ep_0", [(k, k + reach) for k in range(chips - reach)])
        if reach == 1:
            before, total, pay = call(
                start_body, [carry, carry, pay_shape], total, got, name="scan"
            )
        elif reach * 2 < chips:
            before, total, pay = call(
                chain_body, [carry, carry, pay_shape], before, total, got, name="scan"
            )
        reach *= 2
    return pl.pallas_call(head_body, in_specs=smem(6), out_shape=shaped((count, HEAD), BF), name="head")(
        core, base, q_decayed, before, got, other, gates
    )


def exchanged_weights(down_proj, out_weight, lane):
    peers = lax.axis_size("tp_1")
    rows = lax.axis_size("tp_0")
    down = down_proj.reshape(rows, peers, -1, HEAD)
    heads = out_weight.reshape(rows, peers, -1, HEAD)

    def block(at):
        return jnp.concatenate(
            [lax.dynamic_index_in_dim(part, at, 1, keepdims=False) for part in (down, heads)], axis=1
        )

    found = [block(lane)]
    for far in range(1, peers):
        found.append(
            lax.ppermute(
                block((lane + far) % peers), "tp_1", [(k, (k + far) % peers) for k in range(peers)]
            )
        )
    return found


def on_device(
    queries,
    keys,
    values,
    gates,
    log_decay,
    out_weight,
    moe_rows,
    moe_gain,
    routes,
    route_weights,
    gate_proj,
    up_proj,
    down_proj,
):
    experts = lax.axis_size(EP)
    tokens = moe_rows.shape[0]
    lane = lax.axis_index("tp_1")
    send, slots = dispatch(moe_rows, moe_gain, routes, experts, lax.axis_index(TP).reshape(1))
    weights = exchanged_weights(down_proj, out_weight, lane)
    arrived = lax.all_to_all(send, EP, 0, 0, tiled=True)
    count = experts * arrived.shape[1]
    members = lax.axis_size(TP)
    spread = jnp.broadcast_to(arrived.reshape(1, count, HEAD), (members, count, HEAD))
    rows = lax.all_to_all(spread, TP, 0, 0, tiled=True)
    head_out = retention_heads(queries, keys, values, gates, log_decay)
    mixed = hidden_stage(rows, gate_proj, up_proj, head_out, lax.axis_size("tp_0"))
    got = lax.all_to_all(mixed, "tp_0", 0, 0, tiled=True)
    partial = project_stage(lane.reshape(1), got, weights)
    pieces = lax.all_to_all(partial, "tp_1", 0, 0, tiled=True)
    summed = jnp.sum(pieces.astype(F32), axis=0).astype(BF)
    mixer_out = summed[count:]
    back = lax.all_to_all(
        summed[:count].reshape(experts, -1, HEAD), EP, 0, 0, tiled=True
    )
    moe_out = call(
        combine_body, shaped((tokens, HEAD), BF), back, slots.T, route_weights, name="combine"
    )
    return (mixer_out, moe_out)


def solution(mesh):
    torus = Mesh(mesh.devices.reshape(16, 2, 4, 4), ("ep_0", "ep_1", "tp_0", "tp_1"))
    return jax.shard_map(
        on_device,
        mesh=torus,
        in_specs=(
            P(EP, TP),
            P(EP, TP),
            P(EP, TP),
            P(EP, TP),
            P(EP, TP),
            P(None, TP),
            P(EP, None),
            P(),
            P(EP, None),
            P(EP, None),
            P(EP, None, TP),
            P(EP, None, TP),
            P(EP, None, TP),
        ),
        out_specs=(P(EP, TP), P(EP, TP)),
        check_vma=False,
    )
```

```python
import jax
import jax.numpy as jnp
from jax import lax
from jax.experimental import pallas as pl
from jax.experimental.pallas import tpu as pltpu
from jax.sharding import Mesh
from jax.sharding import PartitionSpec as P

BLOCK = 128
HEAD = 128
EP = ("ep_0", "ep_1")
TP = ("tp_0", "tp_1")
BF = jnp.bfloat16
F32 = jnp.float32
HIGH = lax.Precision.HIGHEST
PAY = HEAD + 16
LIMIT = 12 * 1024 * 1024


def dot(a, b, dims=((1,), (0,)), precision=None):
    return lax.dot_general(a, b, (dims, ((), ())), precision=precision, preferred_element_type=F32)


def shaped(shape, dtype):
    return jax.ShapeDtypeStruct(shape, dtype)


def onchip(shape, dtype):
    return pltpu.VMEM(shape, dtype)


def call(body, out_shape, *args, scalars=0, far=0, scratch=()):
    near = len(args) - far
    held = [
        arg if k < scalars or k >= near else pltpu.with_memory_space_constraint(arg, pltpu.VMEM)
        for k, arg in enumerate(args)
    ]
    specs = [
        pl.BlockSpec(memory_space=pltpu.SMEM)
        if k < scalars
        else pl.BlockSpec(memory_space=pltpu.VMEM if k < near else pl.ANY)
        for k in range(len(args))
    ]
    single = not isinstance(out_shape, (list, tuple))
    outs = pl.BlockSpec(memory_space=pltpu.VMEM)
    return pl.pallas_call(
        body,
        in_specs=specs,
        out_specs=outs if single else [outs] * len(out_shape),
        out_shape=out_shape,
        scratch_shapes=list(scratch),
        compiler_params=pltpu.CompilerParams(vmem_limit_bytes=LIMIT),
    )(*held)


def route_body(turn, routes, rows, part, gain, send, slots):
    tokens = rows.shape[0]
    experts = send.shape[0]
    room = send.shape[1]
    wide = rows[...].astype(F32)
    power = jnp.mean(wide * wide, axis=-1, keepdims=True)
    normed = (part[...].astype(F32) * lax.rsqrt(power + 1e-06) * gain[...].astype(F32)).astype(BF)
    first = routes[0:1, :]
    second = routes[1:2, :]
    expert = lax.broadcasted_iota(jnp.int32, (experts, tokens), 0)
    is_first = expert == first
    is_second = expert == second
    named = jnp.where(is_first | is_second, 1.0, 0.0).astype(BF)
    earlier = lax.broadcasted_iota(jnp.int32, (tokens, tokens), 0) < lax.broadcasted_iota(
        jnp.int32, (tokens, tokens), 1
    )
    rank = dot(named, jnp.where(earlier, 1.0, 0.0).astype(BF)).astype(jnp.int32)
    slot_a = first * room + jnp.sum(jnp.where(is_first, rank, 0), axis=0, keepdims=True)
    slot_b = second * room + jnp.sum(jnp.where(is_second, rank, 0), axis=0, keepdims=True)
    slots[0:1, :] = slot_a
    slots[1:2, :] = slot_b
    place = lax.broadcasted_iota(jnp.int32, (experts * room, tokens), 0)
    chosen = jnp.where((place == slot_a) | (place == slot_b), 1.0, 0.0).astype(BF)
    send[...] = dot(chosen, normed).astype(BF).reshape(experts, room, HEAD)


def dispatch(moe_rows, moe_gain, routes, experts, turn):
    tokens, width = moe_rows.shape
    room = 2 * tokens // experts
    grid = pltpu.PrefetchScalarGridSpec(
        num_scalar_prefetch=1,
        grid=(1,),
        in_specs=[
            pl.BlockSpec((2, tokens), lambda i, t: (0, 0)),
            pl.BlockSpec((tokens, width), lambda i, t: (0, 0)),
            pl.BlockSpec((tokens, HEAD), lambda i, t: (0, t[0])),
            pl.BlockSpec((1, HEAD), lambda i, t: (0, t[0])),
        ],
        out_specs=[
            pl.BlockSpec((experts, room, HEAD), lambda i, t: (0, 0, 0)),
            pl.BlockSpec((2, tokens), lambda i, t: (0, 0)),
        ],
    )
    return pl.pallas_call(
        route_body,
        grid_spec=grid,
        out_shape=[shaped((experts, room, HEAD), BF), shaped((2, tokens), jnp.int32)],
        name="route",
        compiler_params=pltpu.CompilerParams(vmem_limit_bytes=LIMIT),
    )(turn, routes.T, moe_rows, moe_rows, moe_gain.reshape(1, width))


def spread_body(rows, out):
    flat = rows[...].reshape(out.shape[1], HEAD)
    for k in range(out.shape[0]):
        out[k] = flat


def hidden_body(rows, w_gate, w_up, out):
    parts, count, _ = rows.shape
    gate = jnp.zeros((count, w_gate.shape[2]), F32)
    up = gate
    for k in range(0, parts, 2):
        left = jnp.concatenate([rows[k], rows[k + 1]], axis=1)
        span = slice(k * HEAD, (k + 2) * HEAD)
        gate += dot(left, w_gate[0, span, :])
        up += dot(left, w_up[0, span, :])
    hidden = (gate / (1.0 + jnp.exp(-gate)) * up).astype(BF)
    for k in range(out.shape[0]):
        out[k, 0:count, :] = hidden[:, 0:HEAD]
        out[k, count:, :] = hidden[:, HEAD:]


def down_body(lane, got, w_0, w_1, w_2, w_3, out):
    peers = got.shape[0]
    count = got.shape[1] // 2
    left = [
        jnp.concatenate([got[k, 0:count, :], got[k, count:, :]], axis=1) for k in range(peers)
    ]
    for first, (one, two) in ((0, (w_0, w_1)), (2, (w_2, w_3))):
        expert = jnp.zeros((count, 2 * HEAD), F32)
        for k in range(peers):
            both = jnp.concatenate([one[k, 0 : 2 * HEAD], two[k, 0 : 2 * HEAD]], axis=1)
            expert += dot(left[k], both)
        for which in range(2):
            at = (lane[0] + peers - first - which) % peers
            cols = slice(which * HEAD, which * HEAD + HEAD)
            out[pl.ds(at, 1)] = expert[:, cols].astype(BF)[None]


def mix_body(own, h_1, h_2, h_3, w_0, w_1, w_2, w_3, row, o_0, o_1, o_2, o_3):
    peers = 4
    heads = [own[...], h_1[...], h_2[...], h_3[...]]
    for (one, two), (put, put_b) in (((w_0, w_1), (o_0, o_1)), ((w_2, w_3), (o_2, o_3))):
        mixer = jnp.zeros((own.shape[0], 2 * HEAD), F32)
        for far in range(peers):
            at = (row[0] + peers - far) % peers
            both = jnp.concatenate(
                [one[pl.ds(at, 1), 2 * HEAD :][0], two[pl.ds(at, 1), 2 * HEAD :][0]], axis=1
            )
            mixer += dot(heads[far], both)
        put[...] = mixer[:, 0:HEAD].astype(BF)
        put_b[...] = mixer[:, HEAD:].astype(BF)


def add_body(parts, out):
    total = parts[0].astype(F32)
    for k in range(1, parts.shape[0]):
        total += parts[k].astype(F32)
    out[...] = total.astype(BF).reshape(out.shape)


def add_four_body(p_0, p_1, p_2, p_3, out):
    out[...] = (
        (p_0[...].astype(F32) + p_1[...].astype(F32))
        + (p_2[...].astype(F32) + p_3[...].astype(F32))
    ).astype(BF)


def combine_body(back, slots, weights, out):
    experts, room, _ = back.shape
    rows = back[...].reshape(experts * room, HEAD)
    tokens = slots.shape[0]
    place = lax.broadcasted_iota(jnp.int32, (tokens, experts * room), 1)
    total = jnp.zeros((tokens, HEAD), F32)
    for k in range(2):
        chosen = jnp.where(place == slots[:, k : k + 1], 1.0, 0.0).astype(BF)
        total += dot(chosen, rows) * weights[:, k : k + 1]
    out[...] = total.astype(BF)


def local_body(q, k, v, decay, cosine, sine, base, q_decayed, state, pay):
    count = q.shape[0]
    blocks = count // BLOCK
    cos = cosine[...]
    sin = sine[...]
    rows = lax.broadcasted_iota(jnp.int32, (BLOCK, BLOCK), 0)
    cols = lax.broadcasted_iota(jnp.int32, (BLOCK, BLOCK), 1)
    causal = rows >= cols
    upper = jnp.where(rows <= cols, 1.0, 0.0)
    lower = jnp.where(causal, 1.0, 0.0)

    def turned(x, factor):
        wide = x.astype(F32)
        swapped = pltpu.roll(wide, HEAD // 2, 1)
        return ((wide * cos + swapped * sin) * factor).astype(BF)

    q_all = turned(q[...], 1.0)
    k_all = turned(k[...], HEAD ** (-0.5))
    carried = jnp.zeros((HEAD, HEAD), F32)
    leading = jnp.zeros((1, HEAD), F32)
    for n in range(blocks):
        span = slice(n * BLOCK, n * BLOCK + BLOCK)
        q_b, k_b, v_b = q_all[span], k_all[span], v[span, :]
        here = jnp.broadcast_to(decay[n : n + 1, :], (BLOCK, BLOCK))
        cum_i = dot(lower, here, ((1,), (1,)), HIGH)
        cum_j = dot(here, upper, precision=HIGH)
        weights = jnp.where(causal, jnp.exp(jnp.where(causal, cum_i - cum_j, 0.0)), 0.0)
        scores = dot(q_b, k_b, ((1,), (1,)))
        inside = dot((scores * weights).astype(BF), v_b)
        q_f = q_b.astype(F32)
        q_d = q_f * jnp.exp(cum_i)
        if n:
            inside += dot(q_d, carried, precision=HIGH)
        base[span, :] = inside
        q_decayed[span, :] = q_f * jnp.exp(cum_i + leading)
        ending = cum_i[BLOCK - 1 : BLOCK, :]
        k_scaled = k_b.astype(F32) * jnp.exp(ending - cum_i)
        update = dot(k_scaled, v_b.astype(F32), ((0,), (0,)), HIGH)
        carried = jnp.exp(ending) * carried + update
        leading = leading + ending
    state[0:HEAD, :] = carried
    state[HEAD:, :] = jnp.broadcast_to(leading, (8, HEAD))
    packed(pay, carried, leading)


def packed(pay, state, total):
    pay[0:HEAD, :] = state.astype(BF)
    high = total.astype(BF)
    rest = total - high.astype(F32)
    middle = rest.astype(BF)
    low = (rest - middle.astype(F32)).astype(BF)
    row = lax.broadcasted_iota(jnp.int32, (16, HEAD), 0)
    three = jnp.where(
        row == 0,
        high.astype(F32),
        jnp.where(row == 1, middle.astype(F32), jnp.where(row == 2, low.astype(F32), 0.0)),
    )
    pay[HEAD:, :] = three.astype(BF)


def unpacked(pay):
    tail = pay[HEAD:, :].astype(F32)
    return pay[0:HEAD, :].astype(F32), tail[0:1] + tail[1:2] + tail[2:3]


def pair_body(core, own, both, other, total, pay):
    state, decay = own[0:HEAD, :], own[HEAD : HEAD + 1, :]
    second = core[0] == 1
    theirs = jnp.where(second, both[0].astype(F32), both[1].astype(F32))
    other[...] = theirs.astype(BF)
    state_o = theirs[0:HEAD]
    decay_o = theirs[HEAD : HEAD + 1] + theirs[HEAD + 1 : HEAD + 2] + theirs[HEAD + 2 : HEAD + 3]
    early = jnp.where(second, state_o, state)
    late = jnp.where(second, state, state_o)
    late_decay = jnp.where(second, decay, decay_o)
    joined = late + jnp.exp(late_decay) * early
    whole = decay + decay_o
    total[0:HEAD, :] = joined
    total[HEAD:, :] = jnp.broadcast_to(whole, (8, HEAD))
    packed(pay, joined, whole)


def chain_body(before, total, got, before_out, total_out, pay):
    state, decay = unpacked(got)
    behind, behind_decay = before[0:HEAD, :], before[HEAD : HEAD + 1, :]
    before_out[0:HEAD, :] = behind + jnp.exp(behind_decay) * state
    before_out[HEAD:, :] = jnp.broadcast_to(behind_decay + decay, (8, HEAD))
    mine, mine_decay = total[0:HEAD, :], total[HEAD : HEAD + 1, :]
    joined = mine + jnp.exp(mine_decay) * state
    whole = mine_decay + decay
    total_out[0:HEAD, :] = joined
    total_out[HEAD:, :] = jnp.broadcast_to(whole, (8, HEAD))
    packed(pay, joined, whole)


def start_body(total, got, before_out, total_out, pay):
    state, decay = unpacked(got)
    before_out[0:HEAD, :] = state
    before_out[HEAD:, :] = jnp.broadcast_to(decay, (8, HEAD))
    mine, mine_decay = total[0:HEAD, :], total[HEAD : HEAD + 1, :]
    joined = mine + jnp.exp(mine_decay) * state
    whole = mine_decay + decay
    total_out[0:HEAD, :] = joined
    total_out[HEAD:, :] = jnp.broadcast_to(whole, (8, HEAD))
    packed(pay, joined, whole)


def head_body(core, base, q_decayed, before, got, other, gates, out):
    state, _ = unpacked(got)
    behind, behind_decay = before[0:HEAD, :], before[HEAD : HEAD + 1, :]
    entering = behind + jnp.exp(behind_decay) * state
    state_o, decay_o = unpacked(other)
    entering = jnp.where(core[0] == 1, state_o + jnp.exp(decay_o) * entering, entering)
    retained = base[...] + dot(q_decayed[...], entering, precision=HIGH)
    power = jnp.mean(retained * retained, axis=-1, keepdims=True)
    gate = gates[...].astype(F32)
    out[...] = (retained * lax.rsqrt(power + 1e-05) * (gate / (1.0 + jnp.exp(-gate)))).astype(BF)


def retention_heads(queries, keys, values, gates, log_decay):
    count = queries.shape[0]
    positions = (lax.axis_index(EP) * count + jnp.arange(count, dtype=jnp.int32)).astype(F32)
    half = HEAD // 2
    inverse = 10000.0 ** (-jnp.arange(half, dtype=F32) / half)
    angles = positions[:, None] * jnp.concatenate([inverse, inverse])[None, :]
    cosine = jnp.cos(angles)
    sine = jnp.sin(angles) * jnp.where(jnp.arange(HEAD) < half, -1.0, 1.0)[None, :]
    carry = onchip((HEAD + 8, HEAD), F32)
    pay_shape = onchip((PAY, HEAD), BF)
    flat = onchip((count, HEAD), F32)
    core = lax.axis_index("ep_1").reshape(1)
    base, q_decayed, own, pay = call(
        local_body,
        [flat, flat, carry, pay_shape],
        queries,
        keys,
        values,
        log_decay.reshape(count // BLOCK, BLOCK),
        cosine,
        sine,
    )
    both = lax.all_gather(pay, "ep_1")
    other, total, pay = call(pair_body, [pay_shape, carry, pay_shape], core, own, both, scalars=1)
    chips = lax.axis_size("ep_0")
    before = None
    reach = 1
    while reach < chips:
        got = lax.ppermute(pay, "ep_0", [(k, k + reach) for k in range(chips - reach)])
        if reach == 1:
            before, total, pay = call(start_body, [carry, carry, pay_shape], total, got)
        elif reach * 2 < chips:
            before, total, pay = call(chain_body, [carry, carry, pay_shape], before, total, got)
        reach *= 2
    return call(
        head_body,
        onchip((count, HEAD), BF),
        core,
        base,
        q_decayed,
        before,
        got,
        other,
        gates,
        scalars=1,
    )


def cut_body(lane, down, heads, *rest):
    peers = len(rest) - 1
    outs, sems = rest[:peers], rest[peers]
    units = down.shape[2]
    copies = []
    for far in range(peers):
        at = (lane[0] + far) % peers
        copies.append(
            pltpu.make_async_copy(down.at[:, at], outs[far].at[:, 0:units], sems.at[2 * far])
        )
        copies.append(
            pltpu.make_async_copy(heads.at[:, at], outs[far].at[:, units:], sems.at[2 * far + 1])
        )
    for copy in copies:
        copy.start()
    for copy in copies:
        copy.wait()


def shifted(array, axis, far):
    peers = lax.axis_size(axis)
    return lax.ppermute(array, axis, [(k, (k + far) % peers) for k in range(peers)])


def exchanged_weights(down_proj, out_weight, lane):
    peers = lax.axis_size("tp_1")
    rows = lax.axis_size("tp_0")
    down = down_proj.reshape(rows, peers, -1, HEAD)
    heads = out_weight.reshape(rows, peers, -1, HEAD)
    tall = down.shape[2] + heads.shape[2]
    found = call(
        cut_body,
        [onchip((rows, tall, HEAD), BF)] * peers,
        lane.reshape(1),
        down,
        heads,
        scalars=1,
        far=2,
        scratch=[pltpu.SemaphoreType.DMA((2 * peers,))],
    )
    swapped = [found[0]]
    for far in range(1, peers):
        swapped.append(shifted(found[far], "tp_1", far))
    return swapped


def both_halves(
    queries,
    keys,
    values,
    gates,
    log_decay,
    out_weight,
    moe_rows,
    moe_gain,
    routes,
    route_weights,
    gate_proj,
    up_proj,
    down_proj,
):
    experts = lax.axis_size(EP)
    members = lax.axis_size(TP)
    tokens = moe_rows.shape[0]
    positions = queries.shape[0]
    lane = lax.axis_index("tp_1")
    row = lax.axis_index("tp_0").reshape(1)
    room = 2 * tokens // experts
    count = experts * room
    rows_y = lax.axis_size("tp_0")
    peers = lax.axis_size("tp_1")
    send, slots = dispatch(moe_rows, moe_gain, routes, experts, lax.axis_index(TP).reshape(1))
    weights = exchanged_weights(down_proj, out_weight, lane)
    arrived = lax.all_to_all(send, EP, 0, 0, tiled=True)
    spread = call(spread_body, onchip((members, count, HEAD), BF), arrived)
    rows = lax.all_to_all(spread, TP, 0, 0, tiled=True)
    head_out = retention_heads(queries, keys, values, gates, log_decay)
    mixed = call(hidden_body, onchip((rows_y, 2 * count, HEAD), BF), rows, gate_proj, up_proj)
    got = lax.all_to_all(mixed, "tp_0", 0, 0, tiled=True)
    heads = [head_out]
    for far in range(1, rows_y):
        heads.append(shifted(head_out, "tp_0", far))
    partial = call(
        down_body, onchip((peers, count, HEAD), BF), lane.reshape(1), got, *weights, scalars=1
    )
    pieces = lax.all_to_all(partial, "tp_1", 0, 0, tiled=True)
    mixes = mix_call(heads, weights, row, positions)
    summed = call(add_body, onchip((experts, room, HEAD), BF), pieces)
    back = lax.all_to_all(summed, EP, 0, 0, tiled=True)
    gathered = [mixes[0]]
    for far in range(1, peers):
        gathered.append(shifted(mixes[far], "tp_1", peers - far))
    mixer_out = call(add_four_body, shaped((positions, HEAD), BF), *gathered)
    columns, scales = lax.optimization_barrier((slots.T, route_weights))
    moe_out = call(combine_body, shaped((tokens, HEAD), BF), back, columns, scales)
    return (mixer_out, moe_out)


def mix_call(heads, weights, row, positions):
    args = [*heads, *weights]
    held = [pltpu.with_memory_space_constraint(arg, pltpu.VMEM) for arg in args]
    near = pl.BlockSpec(memory_space=pltpu.VMEM)
    return pl.pallas_call(
        mix_body,
        in_specs=[near] * len(held) + [pl.BlockSpec(memory_space=pltpu.SMEM)],
        out_specs=[near] * 4,
        out_shape=[onchip((positions, HEAD), BF)] * 4,
        name="mix",
        compiler_params=pltpu.CompilerParams(vmem_limit_bytes=LIMIT),
    )(*held, row)


def solution(mesh):
    torus = Mesh(mesh.devices.reshape(16, 2, 4, 4), ("ep_0", "ep_1", "tp_0", "tp_1"))
    return jax.shard_map(
        both_halves,
        mesh=torus,
        in_specs=(
            P(EP, TP),
            P(EP, TP),
            P(EP, TP),
            P(EP, TP),
            P(EP, TP),
            P(None, TP),
            P(EP, None),
            P(),
            P(EP, None),
            P(EP, None),
            P(EP, None, TP),
            P(EP, None, TP),
            P(EP, None, TP),
        ),
        out_specs=(P(EP, TP), P(EP, TP)),
        check_vma=False,
    )
```

```python
import functools

import jax
import jax.numpy as jnp
from jax import lax
from jax.experimental import pallas as pl
from jax.experimental.pallas import tpu as pltpu
from jax.sharding import Mesh
from jax.sharding import PartitionSpec as P

BLOCK = 128
HEAD = 128
EP = ("ep_0", "ep_1")
TP = ("tp_0", "tp_1")
BF = jnp.bfloat16
F32 = jnp.float32
HIGH = lax.Precision.HIGHEST
PAY = HEAD + 16
LIMIT = 12 * 1024 * 1024


def dot(a, b, dims=((1,), (0,)), precision=None):
    return lax.dot_general(a, b, (dims, ((), ())), precision=precision, preferred_element_type=F32)


def shaped(shape, dtype):
    return jax.ShapeDtypeStruct(shape, dtype)


def onchip(shape, dtype):
    return pltpu.VMEM(shape, dtype)


def call(body, out_shape, *args, kinds, outs="v", scratch=()):
    places = {
        "s": pl.BlockSpec(memory_space=pltpu.SMEM),
        "v": pl.BlockSpec(memory_space=pltpu.VMEM),
        "h": pl.BlockSpec(),
        "p": pl.BlockSpec(),
        "a": pl.BlockSpec(memory_space=pltpu.HBM),
    }
    held = [
        pltpu.with_memory_space_constraint(arg, {"v": pltpu.VMEM}.get(kind, pltpu.HBM))
        if kind in "vpa"
        else arg
        for arg, kind in zip(args, kinds, strict=True)
    ]
    single = not isinstance(out_shape, (list, tuple))
    out_specs = [places[kind] for kind in outs]
    return pl.pallas_call(
        body,
        in_specs=[places[kind] for kind in kinds],
        out_specs=out_specs[0] if single else out_specs,
        out_shape=out_shape,
        scratch_shapes=list(scratch),
        compiler_params=pltpu.CompilerParams(vmem_limit_bytes=LIMIT),
    )(*held)


def route_body(turn, routes, gain, source, send, slots, rows, sems):
    tokens = rows.shape[0]
    experts = send.shape[0]
    room = send.shape[1]
    chunks = sems.shape[0]
    tall = tokens // chunks
    copies = [
        pltpu.make_async_copy(
            source.at[pl.ds(k * tall, tall)], rows.at[pl.ds(k * tall, tall)], sems.at[k]
        )
        for k in range(chunks)
    ]
    for copy in copies:
        copy.start()
    first = routes[0:1, :]
    second = routes[1:2, :]
    expert = lax.broadcasted_iota(jnp.int32, (experts, tokens), 0)
    is_first = expert == first
    is_second = expert == second
    named = jnp.where(is_first | is_second, 1.0, 0.0).astype(BF)
    earlier = lax.broadcasted_iota(jnp.int32, (tokens, tokens), 0) < lax.broadcasted_iota(
        jnp.int32, (tokens, tokens), 1
    )
    rank = dot(named, jnp.where(earlier, 1.0, 0.0).astype(BF)).astype(jnp.int32)
    slot_a = first * room + jnp.sum(jnp.where(is_first, rank, 0), axis=0, keepdims=True)
    slot_b = second * room + jnp.sum(jnp.where(is_second, rank, 0), axis=0, keepdims=True)
    slots[0:1, :] = slot_a
    slots[1:2, :] = slot_b
    place = lax.broadcasted_iota(jnp.int32, (experts * room, tokens), 0)
    chosen = jnp.where((place == slot_a) | (place == slot_b), 1.0, 0.0).astype(BF)
    which = lax.broadcasted_iota(jnp.int32, gain.shape, 0) == turn[0]
    scale = jnp.sum(jnp.where(which, gain[...].astype(F32), 0.0), axis=0, keepdims=True)
    at = pl.multiple_of(turn[0] * HEAD, HEAD)
    parts = []
    for k, copy in enumerate(copies):
        copy.wait()
        wide = rows[k * tall : (k + 1) * tall, :].astype(F32)
        power = jnp.mean(wide * wide, axis=-1, keepdims=True)
        part = rows[k * tall : (k + 1) * tall, pl.ds(at, HEAD)].astype(F32)
        parts.append((part * lax.rsqrt(power + 1e-06) * scale).astype(BF))
    normed = jnp.concatenate(parts, axis=0)
    send[...] = dot(chosen, normed).astype(BF).reshape(experts, room, HEAD)


def dispatch(moe_rows, moe_gain, routes, experts, turn):
    tokens, width = moe_rows.shape
    room = 2 * tokens // experts
    return call(
        route_body,
        [onchip((experts, room, HEAD), BF), onchip((2, tokens), jnp.int32)],
        turn,
        routes.T,
        moe_gain.reshape(width // HEAD, HEAD),
        moe_rows,
        kinds="sppa",
        outs="vv",
        scratch=[pltpu.VMEM((tokens, width), BF), pltpu.SemaphoreType.DMA((4,))],
    )


def spread_body(rows, out, sems):
    copies = [pltpu.make_async_copy(rows, out.at[k], sems.at[k]) for k in range(out.shape[0])]
    for copy in copies:
        copy.start()
    for copy in copies:
        copy.wait()


def hidden_body(rows, heads, w_gate, w_up, out, near_gate, near_up, sems):
    parts, count, _ = rows.shape
    chunks = sems.shape[1]
    tall = w_gate.shape[1] // chunks
    copies = []
    for k in range(chunks):
        span = pl.ds(k * tall, tall)
        copies.append(
            (
                pltpu.make_async_copy(w_gate.at[0, span], near_gate.at[span], sems.at[0, k]),
                pltpu.make_async_copy(w_up.at[0, span], near_up.at[span], sems.at[1, k]),
            )
        )
    for one, two in copies:
        one.start()
        two.start()
    gate = jnp.zeros((count, w_gate.shape[2]), F32)
    up = gate
    per = parts // chunks
    for k in range(chunks):
        left = jnp.concatenate([rows[k * per + j] for j in range(per)], axis=1)
        span = slice(k * tall, (k + 1) * tall)
        copies[k][0].wait()
        gate += dot(left, near_gate[span, :])
        copies[k][1].wait()
        up += dot(left, near_up[span, :])
    hidden = (gate / (1.0 + jnp.exp(-gate)) * up).astype(BF)
    for k in range(out.shape[0]):
        out[k, 0:count, :] = hidden[:, 0:HEAD]
        out[k, count : 2 * count, :] = hidden[:, HEAD:]
        out[k, 2 * count :, :] = heads[...]


def project_body(lane, got, w_0, w_1, w_2, w_3, out, n_0, n_1, n_2, n_3, sems):
    peers = got.shape[0]
    positions = got.shape[1] // 5
    count = 2 * positions
    units = 2 * HEAD
    near = (n_0, n_1, n_2, n_3)
    copies = [
        pltpu.make_async_copy(far, here, sems.at[k])
        for k, (far, here) in enumerate(zip((w_0, w_1, w_2, w_3), near, strict=True))
    ]
    for copy in copies:
        copy.start()
    left = [
        jnp.concatenate([got[k, 0:count, :], got[k, count : 2 * count, :]], axis=1)
        for k in range(peers)
    ]
    for first in (0, 2):
        one, two = near[first], near[first + 1]
        copies[first].wait()
        copies[first + 1].wait()
        expert = jnp.zeros((count, 2 * HEAD), F32)
        mixer = jnp.zeros((positions, 2 * HEAD), F32)
        for k in range(peers):
            both = jnp.concatenate([one[k], two[k]], axis=1)
            expert += dot(left[k], both[0:units])
            mixer += dot(got[k, 2 * count :, :], both[units:])
        for which in range(2):
            at = (lane[0] + peers - first - which) % peers
            cols = slice(which * HEAD, which * HEAD + HEAD)
            out[pl.ds(at, 1), 0:count, :] = expert[:, cols].astype(BF)[None]
            out[pl.ds(at, 1), count:, :] = mixer[:, cols].astype(BF)[None]


def add_body(parts, experts, mixer):
    total = parts[0].astype(F32)
    for k in range(1, parts.shape[0]):
        total += parts[k].astype(F32)
    count = experts.shape[0] * experts.shape[1]
    experts[...] = total[0:count].astype(BF).reshape(experts.shape)
    mixer[...] = total[count:].astype(BF)


def combine_body(back, slots, weights, out):
    experts, room, _ = back.shape
    rows = back[...].reshape(experts * room, HEAD)
    tokens = slots.shape[0]
    place = lax.broadcasted_iota(jnp.int32, (tokens, experts * room), 1)
    total = jnp.zeros((tokens, HEAD), F32)
    for k in range(2):
        chosen = jnp.where(place == slots[:, k : k + 1], 1.0, 0.0).astype(BF)
        total += dot(chosen, rows) * weights[:, k : k + 1]
    out[...] = total.astype(BF)


def local_body(q, k, v, decay, cosine, sine, base, q_decayed, pay):
    count = q.shape[0]
    blocks = count // BLOCK
    cos = cosine[...]
    sin = sine[...]
    rows = lax.broadcasted_iota(jnp.int32, (BLOCK, BLOCK), 0)
    cols = lax.broadcasted_iota(jnp.int32, (BLOCK, BLOCK), 1)
    causal = rows >= cols
    upper = jnp.where(rows <= cols, 1.0, 0.0)
    lower = jnp.where(causal, 1.0, 0.0)

    def turned(x, factor):
        wide = x.astype(F32)
        swapped = pltpu.roll(wide, HEAD // 2, 1)
        return ((wide * cos + swapped * sin) * factor).astype(BF)

    q_all = turned(q[...], 1.0)
    k_all = turned(k[...], HEAD ** (-0.5))
    carried = jnp.zeros((HEAD, HEAD), F32)
    leading = jnp.zeros((1, HEAD), F32)
    for n in range(blocks):
        span = slice(n * BLOCK, n * BLOCK + BLOCK)
        q_b, k_b, v_b = q_all[span], k_all[span], v[span, :]
        here = jnp.broadcast_to(decay[n : n + 1, :], (BLOCK, BLOCK))
        cum_i = dot(lower, here, ((1,), (1,)), HIGH)
        cum_j = dot(here, upper, precision=HIGH)
        weights = jnp.where(causal, jnp.exp(jnp.where(causal, cum_i - cum_j, 0.0)), 0.0)
        scores = dot(q_b, k_b, ((1,), (1,)))
        inside = dot((scores * weights).astype(BF), v_b)
        q_f = q_b.astype(F32)
        q_d = q_f * jnp.exp(cum_i)
        if n:
            inside += dot(q_d, carried, precision=HIGH)
        base[span, :] = inside
        q_decayed[span, :] = q_f * jnp.exp(cum_i + leading)
        ending = cum_i[BLOCK - 1 : BLOCK, :]
        k_scaled = k_b.astype(F32) * jnp.exp(ending - cum_i)
        update = dot(k_scaled, v_b.astype(F32), ((0,), (0,)), HIGH)
        carried = jnp.exp(ending) * carried + update
        leading = leading + ending
    packed(pay, carried, leading)


def packed(pay, state, total):
    pay[0:HEAD, :] = state.astype(BF)
    high = total.astype(BF)
    rest = total - high.astype(F32)
    middle = rest.astype(BF)
    low = (rest - middle.astype(F32)).astype(BF)
    row = lax.broadcasted_iota(jnp.int32, (16, HEAD), 0)
    three = jnp.where(
        row == 0,
        high.astype(F32),
        jnp.where(row == 1, middle.astype(F32), jnp.where(row == 2, low.astype(F32), 0.0)),
    )
    pay[HEAD:, :] = three.astype(BF)


def unpacked(pay):
    tail = pay[HEAD:, :].astype(F32)
    return pay[0:HEAD, :].astype(F32), tail[0:1] + tail[1:2] + tail[2:3]


def pair_body(both, pay):
    early, early_decay = unpacked(both.at[0])
    late, late_decay = unpacked(both.at[1])
    packed(pay, late + jnp.exp(late_decay) * early, early_decay + late_decay)


def head_body(core, chip, chips, both, base, q_decayed, gates, out):
    entering = jnp.zeros((HEAD, HEAD), F32)
    for k in range(chips.shape[0]):
        state, decay = unpacked(chips.at[k])
        entering = jnp.where(k < chip[0], jnp.exp(decay) * entering + state, entering)
    early, early_decay = unpacked(both.at[0])
    entering = jnp.where(core[0] == 1, early + jnp.exp(early_decay) * entering, entering)
    retained = base[...] + dot(q_decayed[...], entering, precision=HIGH)
    power = jnp.mean(retained * retained, axis=-1, keepdims=True)
    gate = gates[...].astype(F32)
    out[...] = (retained * lax.rsqrt(power + 1e-05) * (gate / (1.0 + jnp.exp(-gate)))).astype(BF)


def retention_heads(queries, keys, values, gates, log_decay):
    count = queries.shape[0]
    positions = (lax.axis_index(EP) * count + jnp.arange(count, dtype=jnp.int32)).astype(F32)
    half = HEAD // 2
    inverse = 10000.0 ** (-jnp.arange(half, dtype=F32) / half)
    angles = positions[:, None] * jnp.concatenate([inverse, inverse])[None, :]
    cosine = jnp.cos(angles)
    sine = jnp.sin(angles) * jnp.where(jnp.arange(HEAD) < half, -1.0, 1.0)[None, :]
    flat = shaped((count, HEAD), F32)
    base, q_decayed, pay = call(
        local_body,
        [flat, flat, onchip((PAY, HEAD), BF)],
        queries,
        keys,
        values,
        log_decay.reshape(count // BLOCK, BLOCK),
        cosine,
        sine,
        kinds="hhhhvv",
        outs="hhv",
    )
    both = lax.all_gather(pay, "ep_1")
    pay = call(pair_body, onchip((PAY, HEAD), BF), both, kinds="v")
    chips = lax.all_gather(pay, "ep_0")
    return call(
        head_body,
        shaped((count, HEAD), BF),
        lax.axis_index("ep_1").reshape(1),
        lax.axis_index("ep_0").reshape(1),
        chips,
        both,
        base,
        q_decayed,
        gates,
        kinds="sshhhhh",
        outs="h",
    )


def cut_body(far, lane, down, heads, *rest):
    peers = down.shape[1]
    outs, sems = rest[: len(far)], rest[len(far)]
    units = down.shape[2]
    copies = []
    for k, step in enumerate(far):
        at = (lane[0] + step) % peers
        copies.append(
            pltpu.make_async_copy(down.at[:, at], outs[k].at[:, 0:units], sems.at[2 * k])
        )
        copies.append(
            pltpu.make_async_copy(heads.at[:, at], outs[k].at[:, units:], sems.at[2 * k + 1])
        )
    for copy in copies:
        copy.start()
    for copy in copies:
        copy.wait()


def shifted(array, axis, far):
    peers = lax.axis_size(axis)
    return lax.ppermute(array, axis, [(k, (k + far) % peers) for k in range(peers)])


def exchanged_weights(down_proj, out_weight, lane):
    peers = lax.axis_size("tp_1")
    rows = lax.axis_size("tp_0")
    down = down_proj.reshape(rows, peers, -1, HEAD)
    heads = out_weight.reshape(rows, peers, -1, HEAD)
    shape = (rows, down.shape[2] + heads.shape[2], HEAD)

    def cut(steps, outs, places):
        return call(
            functools.partial(cut_body, steps),
            outs,
            lane.reshape(1),
            down,
            heads,
            kinds="saa",
            outs=places,
            scratch=[pltpu.SemaphoreType.DMA((2 * len(steps),))],
        )

    one, three = cut((1, 3), [onchip(shape, BF), onchip(shape, BF)], "vv")
    own, two = cut((0, 2), [pltpu.HBM(shape, BF), onchip(shape, BF)], "av")
    swapped = [own]
    for far, block in ((1, one), (2, two), (3, three)):
        swapped.append(shifted(block, "tp_1", far))
    return swapped


def both_halves(
    queries,
    keys,
    values,
    gates,
    log_decay,
    out_weight,
    moe_rows,
    moe_gain,
    routes,
    route_weights,
    gate_proj,
    up_proj,
    down_proj,
):
    experts = lax.axis_size(EP)
    members = lax.axis_size(TP)
    tokens = moe_rows.shape[0]
    positions = queries.shape[0]
    lane = lax.axis_index("tp_1")
    room = 2 * tokens // experts
    count = experts * room
    rows_y = lax.axis_size("tp_0")
    peers = lax.axis_size("tp_1")
    units = gate_proj.shape[2]
    tall = 2 * count + positions
    send, slots = dispatch(moe_rows, moe_gain, routes, experts, lax.axis_index(TP).reshape(1))
    weights = exchanged_weights(down_proj, out_weight, lane)
    arrived = lax.all_to_all(send, EP, 0, 0, tiled=True)
    spread = call(
        spread_body,
        pltpu.HBM((members, count, HEAD), BF),
        arrived.reshape(count, HEAD),
        kinds="v",
        outs="a",
        scratch=[pltpu.SemaphoreType.DMA((members,))],
    )
    rows = lax.all_to_all(spread, TP, 0, 0, tiled=True)
    head_out = retention_heads(queries, keys, values, gates, log_decay)
    width = gate_proj.shape[1]
    mixed = call(
        hidden_body,
        onchip((rows_y, tall, HEAD), BF),
        rows,
        head_out,
        gate_proj,
        up_proj,
        kinds="vhaa",
        scratch=[
            pltpu.VMEM((width, units), BF),
            pltpu.VMEM((width, units), BF),
            pltpu.SemaphoreType.DMA((2, 4)),
        ],
    )
    got = lax.all_to_all(mixed, "tp_0", 0, 0, tiled=True)
    block = pltpu.VMEM(weights[0].shape, BF)
    partial = call(
        project_body,
        onchip((peers, count + positions, HEAD), BF),
        lane.reshape(1),
        got,
        *weights,
        kinds="svaaaa",
        scratch=[block] * peers + [pltpu.SemaphoreType.DMA((peers,))],
    )
    pieces = lax.all_to_all(partial, "tp_1", 0, 0, tiled=True)
    summed, mixer_out = call(
        add_body,
        [onchip((experts, room, HEAD), BF), shaped((positions, HEAD), BF)],
        pieces,
        kinds="v",
        outs="vh",
    )
    back = lax.all_to_all(summed, EP, 0, 0, tiled=True)
    columns, scales = lax.optimization_barrier((slots.T, route_weights))
    moe_out = call(
        combine_body, shaped((tokens, HEAD), BF), back, columns, scales, kinds="vvv", outs="h"
    )
    return (mixer_out, moe_out)


def solution(mesh):
    torus = Mesh(mesh.devices.reshape(16, 2, 4, 4), ("ep_0", "ep_1", "tp_0", "tp_1"))
    return jax.shard_map(
        both_halves,
        mesh=torus,
        in_specs=(
            P(EP, TP),
            P(EP, TP),
            P(EP, TP),
            P(EP, TP),
            P(EP, TP),
            P(None, TP),
            P(EP, None),
            P(),
            P(EP, None),
            P(EP, None),
            P(EP, None, TP),
            P(EP, None, TP),
            P(EP, None, TP),
        ),
        out_specs=(P(EP, TP), P(EP, TP)),
        check_vma=False,
    )
```

```python
import functools

import jax
import jax.numpy as jnp
from jax import lax
from jax.experimental import pallas as pl
from jax.experimental.pallas import tpu as pltpu
from jax.sharding import Mesh
from jax.sharding import PartitionSpec as P

BLOCK = 128
HEAD = 128
EP = ("ep_0", "ep_1", "ep_2")
TP = ("tp_0", "tp_1")
BF = jnp.bfloat16
F32 = jnp.float32
HIGH = lax.Precision.HIGHEST
PAY = HEAD + 16
LIMIT = 12 * 1024 * 1024


def dot(a, b, dims=((1,), (0,)), precision=None):
    return lax.dot_general(a, b, (dims, ((), ())), precision=precision, preferred_element_type=F32)


def shaped(shape, dtype):
    return jax.ShapeDtypeStruct(shape, dtype)


def onchip(shape, dtype):
    return pltpu.VMEM(shape, dtype)


def call(body, out_shape, *args, kinds, outs="v", scratch=()):
    places = {
        "s": pl.BlockSpec(memory_space=pltpu.SMEM),
        "v": pl.BlockSpec(memory_space=pltpu.VMEM),
        "h": pl.BlockSpec(),
        "p": pl.BlockSpec(),
        "a": pl.BlockSpec(memory_space=pltpu.HBM),
    }
    held = [
        pltpu.with_memory_space_constraint(arg, {"v": pltpu.VMEM}.get(kind, pltpu.HBM))
        if kind in "vpa"
        else arg
        for arg, kind in zip(args, kinds, strict=True)
    ]
    single = not isinstance(out_shape, (list, tuple))
    out_specs = [places[kind] for kind in outs]
    return pl.pallas_call(
        body,
        in_specs=[places[kind] for kind in kinds],
        out_specs=out_specs[0] if single else out_specs,
        out_shape=out_shape,
        scratch_shapes=list(scratch),
        compiler_params=pltpu.CompilerParams(vmem_limit_bytes=LIMIT),
    )(*held)


def route_body(turn, routes_far, gain_far, source, send, slots, routes, gain, rows, sems, extra):
    tokens = rows.shape[0]
    experts = send.shape[0]
    room = send.shape[1]
    chunks = sems.shape[0]
    tall = tokens // chunks
    copies = [
        pltpu.make_async_copy(
            source.at[pl.ds(k * tall, tall)], rows.at[pl.ds(k * tall, tall)], sems.at[k]
        )
        for k in range(chunks)
    ]
    small = pltpu.make_async_copy(routes_far, routes, extra.at[0])
    scales = pltpu.make_async_copy(gain_far, gain, extra.at[1])
    small.start()
    for copy in copies:
        copy.start()
    scales.start()
    small.wait()
    first = routes[0:1, :]
    second = routes[1:2, :]
    expert = lax.broadcasted_iota(jnp.int32, (experts, tokens), 0)
    is_first = expert == first
    is_second = expert == second
    named = jnp.where(is_first | is_second, 1.0, 0.0).astype(BF)
    earlier = lax.broadcasted_iota(jnp.int32, (tokens, tokens), 0) < lax.broadcasted_iota(
        jnp.int32, (tokens, tokens), 1
    )
    rank = dot(named, jnp.where(earlier, 1.0, 0.0).astype(BF)).astype(jnp.int32)
    slot_a = first * room + jnp.sum(jnp.where(is_first, rank, 0), axis=0, keepdims=True)
    slot_b = second * room + jnp.sum(jnp.where(is_second, rank, 0), axis=0, keepdims=True)
    slots[0:1, :] = slot_a
    slots[1:2, :] = slot_b
    place = lax.broadcasted_iota(jnp.int32, (experts * room, tokens), 0)
    chosen = jnp.where((place == slot_a) | (place == slot_b), 1.0, 0.0).astype(BF)
    scales.wait()
    which = lax.broadcasted_iota(jnp.int32, gain.shape, 0) == turn[0]
    scale = jnp.sum(jnp.where(which, gain[...].astype(F32), 0.0), axis=0, keepdims=True)
    at = pl.multiple_of(turn[0] * HEAD, HEAD)
    parts = []
    for k, copy in enumerate(copies):
        copy.wait()
        wide = rows[k * tall : (k + 1) * tall, :].astype(F32)
        power = jnp.mean(wide * wide, axis=-1, keepdims=True)
        part = rows[k * tall : (k + 1) * tall, pl.ds(at, HEAD)].astype(F32)
        parts.append((part * lax.rsqrt(power + 1e-06) * scale).astype(BF))
    normed = jnp.concatenate(parts, axis=0)
    send[...] = dot(chosen, normed).astype(BF).reshape(experts, room, HEAD)


def dispatch(moe_rows, moe_gain, routes, experts, turn):
    tokens, width = moe_rows.shape
    room = 2 * tokens // experts
    return call(
        route_body,
        [onchip((experts, room, HEAD), BF), onchip((2, tokens), jnp.int32)],
        turn,
        routes.T,
        moe_gain.reshape(width // HEAD, HEAD),
        moe_rows,
        kinds="saaa",
        outs="vv",
        scratch=[
            pltpu.VMEM((2, tokens), jnp.int32),
            pltpu.VMEM((width // HEAD, HEAD), BF),
            pltpu.VMEM((tokens, width), BF),
            pltpu.SemaphoreType.DMA((8,)),
            pltpu.SemaphoreType.DMA((2,)),
        ],
    )


def spread_body(rows, out, sems):
    copies = [pltpu.make_async_copy(rows, out.at[k], sems.at[k]) for k in range(out.shape[0])]
    for copy in copies:
        copy.start()
    for copy in copies:
        copy.wait()


def hidden_body(rows, heads, w_gate, w_up, out, near_gate, near_up, near, sems, ends):
    parts, count, _ = rows.shape
    copied = out.shape[0]
    chunks = sems.shape[1]
    tall = w_gate.shape[1] // chunks
    copies = []
    for k in range(chunks):
        span = pl.ds(k * tall, tall)
        copies.append(
            (
                pltpu.make_async_copy(w_gate.at[0, span], near_gate.at[span], sems.at[0, k]),
                pltpu.make_async_copy(w_up.at[0, span], near_up.at[span], sems.at[1, k]),
            )
        )
    for one, two in copies:
        one.start()
        two.start()
    near[2 * count :, :] = heads[...]
    gate = jnp.zeros((count, w_gate.shape[2]), F32)
    up = gate
    per = parts // chunks
    for k in range(chunks):
        left = jnp.concatenate([rows[k * per + j] for j in range(per)], axis=1)
        span = slice(k * tall, (k + 1) * tall)
        copies[k][0].wait()
        gate += dot(left, near_gate[span, :])
        copies[k][1].wait()
        up += dot(left, near_up[span, :])
    hidden = (gate / (1.0 + jnp.exp(-gate)) * up).astype(BF)
    near[0:count, :] = hidden[:, 0:HEAD]
    near[count : 2 * count, :] = hidden[:, HEAD:]
    final = [pltpu.make_async_copy(near, out.at[k], ends.at[k]) for k in range(copied)]
    for copy in final:
        copy.start()
    for copy in final:
        copy.wait()


def project_body(lane, got, w_0, w_1, w_2, w_3, out):
    peers = got.shape[0]
    positions = got.shape[1] // 5
    count = 2 * positions
    units = 2 * HEAD
    near = (w_0, w_1, w_2, w_3)
    left = [
        jnp.concatenate([got[k, 0:count, :], got[k, count : 2 * count, :]], axis=1)
        for k in range(peers)
    ]
    for first in (0, 2):
        one, two = near[first], near[first + 1]
        expert = jnp.zeros((count, 2 * HEAD), F32)
        mixer = jnp.zeros((positions, 2 * HEAD), F32)
        for k in range(peers):
            both = jnp.concatenate([one[k], two[k]], axis=1)
            expert += dot(left[k], both[0:units])
            mixer += dot(got[k, 2 * count :, :], both[units:])
        for which in range(2):
            at = (lane[0] + peers - first - which) % peers
            cols = slice(which * HEAD, which * HEAD + HEAD)
            out[pl.ds(at, 1), 0:count, :] = expert[:, cols].astype(BF)[None]
            out[pl.ds(at, 1), count:, :] = mixer[:, cols].astype(BF)[None]


def add_body(parts, experts, mixer):
    total = parts[0].astype(F32)
    for k in range(1, parts.shape[0]):
        total += parts[k].astype(F32)
    count = experts.shape[0] * experts.shape[1]
    experts[...] = total[0:count].astype(BF).reshape(experts.shape)
    mixer[...] = total[count:].astype(BF)


def combine_body(back, slots, weights, out):
    experts, room, _ = back.shape
    rows = back[...].reshape(experts * room, HEAD)
    tokens = slots.shape[0]
    place = lax.broadcasted_iota(jnp.int32, (tokens, experts * room), 1)
    total = jnp.zeros((tokens, HEAD), F32)
    for k in range(2):
        chosen = jnp.where(place == slots[:, k : k + 1], 1.0, 0.0).astype(BF)
        total += dot(chosen, rows) * weights[:, k : k + 1]
    out[...] = total.astype(BF)


def local_body(q, k, v, decay, cosine, sine, base, q_decayed, pay):
    count = q.shape[0]
    blocks = count // BLOCK
    cos = cosine[...]
    sin = sine[...]
    rows = lax.broadcasted_iota(jnp.int32, (BLOCK, BLOCK), 0)
    cols = lax.broadcasted_iota(jnp.int32, (BLOCK, BLOCK), 1)
    causal = rows >= cols
    upper = jnp.where(rows <= cols, 1.0, 0.0)
    lower = jnp.where(causal, 1.0, 0.0)

    def turned(x, factor):
        wide = x.astype(F32)
        swapped = pltpu.roll(wide, HEAD // 2, 1)
        return ((wide * cos + swapped * sin) * factor).astype(BF)

    q_all = turned(q[...], 1.0)
    k_all = turned(k[...], HEAD ** (-0.5))
    carried = jnp.zeros((HEAD, HEAD), F32)
    leading = jnp.zeros((1, HEAD), F32)
    for n in range(blocks):
        span = slice(n * BLOCK, n * BLOCK + BLOCK)
        q_b, k_b, v_b = q_all[span], k_all[span], v[span, :]
        here = jnp.broadcast_to(decay[n : n + 1, :], (BLOCK, BLOCK))
        cum_i = dot(lower, here, ((1,), (1,)), HIGH)
        cum_j = dot(here, upper, precision=HIGH)
        weights = jnp.where(causal, jnp.exp(jnp.where(causal, cum_i - cum_j, 0.0)), 0.0)
        scores = dot(q_b, k_b, ((1,), (1,)))
        inside = dot((scores * weights).astype(BF), v_b)
        q_f = q_b.astype(F32)
        q_d = q_f * jnp.exp(cum_i)
        if n:
            inside += dot(q_d, carried, precision=HIGH)
        base[span, :] = inside
        q_decayed[span, :] = q_f * jnp.exp(cum_i + leading)
        ending = cum_i[BLOCK - 1 : BLOCK, :]
        k_scaled = k_b.astype(F32) * jnp.exp(ending - cum_i)
        update = dot(k_scaled, v_b.astype(F32), ((0,), (0,)), HIGH)
        carried = jnp.exp(ending) * carried + update
        leading = leading + ending
    packed(pay, carried, leading)


def packed(pay, state, total):
    pay[0 : state.shape[0], :] = state.astype(BF)
    high = total.astype(BF)
    rest = total - high.astype(F32)
    middle = rest.astype(BF)
    low = (rest - middle.astype(F32)).astype(BF)
    row = lax.broadcasted_iota(jnp.int32, (16, HEAD), 0)
    three = jnp.where(
        row == 0,
        high.astype(F32),
        jnp.where(row == 1, middle.astype(F32), jnp.where(row == 2, low.astype(F32), 0.0)),
    )
    pay[state.shape[0] :, :] = three.astype(BF)


def unpacked(pay):
    rows = pay.shape[0] - 16
    tail = pay[rows:, :].astype(F32)
    return pay[0:rows, :].astype(F32), tail[0:1] + tail[1:2] + tail[2:3]


def quad_body(core, near, pay):
    state, decay = unpacked(near.at[0])
    for k in range(1, near.shape[0]):
        later, later_decay = unpacked(near.at[k])
        state = later + jnp.exp(later_decay) * state
        decay = decay + later_decay
    half = HEAD // 2
    mine = jnp.where(core[0] == 0, state[0:half], state[half:])
    packed(pay, mine, decay)


def head_body(place, group, far, near, base, q_decayed, gates, out):
    entering = jnp.zeros((HEAD, HEAD), F32)
    for k in range(far.shape[0] // 2):
        upper, decay = unpacked(far.at[2 * k])
        lower, _ = unpacked(far.at[2 * k + 1])
        state = jnp.concatenate([upper, lower], axis=0)
        entering = jnp.where(k < group[0], jnp.exp(decay) * entering + state, entering)
    for k in range(near.shape[0] - 1):
        state, decay = unpacked(near.at[k])
        entering = jnp.where(k < place[0], jnp.exp(decay) * entering + state, entering)
    retained = base[...] + dot(q_decayed[...], entering, precision=HIGH)
    power = jnp.mean(retained * retained, axis=-1, keepdims=True)
    gate = gates[...].astype(F32)
    out[...] = (retained * lax.rsqrt(power + 1e-05) * (gate / (1.0 + jnp.exp(-gate)))).astype(BF)


def retention_heads(queries, keys, values, gates, log_decay):
    count = queries.shape[0]
    positions = (lax.axis_index(EP) * count + jnp.arange(count, dtype=jnp.int32)).astype(F32)
    half = HEAD // 2
    inverse = 10000.0 ** (-jnp.arange(half, dtype=F32) / half)
    angles = positions[:, None] * jnp.concatenate([inverse, inverse])[None, :]
    cosine = jnp.cos(angles)
    sine = jnp.sin(angles) * jnp.where(jnp.arange(HEAD) < half, -1.0, 1.0)[None, :]
    flat = pltpu.HBM((count, HEAD), F32)
    base, q_decayed, pay = call(
        local_body,
        [flat, flat, onchip((PAY, HEAD), BF)],
        queries,
        keys,
        values,
        log_decay.reshape(count // BLOCK, BLOCK),
        cosine,
        sine,
        kinds="hhhhvv",
        outs="hhv",
    )
    place = lax.axis_index(("ep_1", "ep_2")).reshape(1)
    near = lax.all_gather(pay, ("ep_1", "ep_2"))
    pay = call(
        quad_body,
        onchip((PAY - HEAD // 2, HEAD), BF),
        lax.axis_index("ep_2").reshape(1),
        near,
        kinds="sv",
    )
    far = lax.all_gather(pay, ("ep_0", "ep_2"))
    return call(
        head_body,
        shaped((count, HEAD), BF),
        place,
        lax.axis_index("ep_0").reshape(1),
        far,
        near,
        base,
        q_decayed,
        gates,
        kinds="sshhpph",
        outs="h",
    )


def cut_body(far, lane, down, heads, *rest):
    peers = down.shape[1]
    outs, sems = rest[: len(far)], rest[len(far)]
    units = down.shape[2]
    copies = []
    for k, step in enumerate(far):
        at = (lane[0] + step) % peers
        copies.append(
            pltpu.make_async_copy(down.at[:, at], outs[k].at[:, 0:units], sems.at[2 * k])
        )
        copies.append(
            pltpu.make_async_copy(heads.at[:, at], outs[k].at[:, units:], sems.at[2 * k + 1])
        )
    for copy in copies:
        copy.start()
    for copy in copies:
        copy.wait()


def shifted(array, axis, far):
    peers = lax.axis_size(axis)
    return lax.ppermute(array, axis, [(k, (k + far) % peers) for k in range(peers)])


def exchanged_weights(down_proj, out_weight, lane):
    peers = lax.axis_size("tp_1")
    rows = lax.axis_size("tp_0")
    down = down_proj.reshape(rows, peers, -1, HEAD)
    heads = out_weight.reshape(rows, peers, -1, HEAD)
    shape = (rows, down.shape[2] + heads.shape[2], HEAD)

    def cut(steps, outs, places):
        return call(
            functools.partial(cut_body, steps),
            outs,
            lane.reshape(1),
            down,
            heads,
            kinds="saa",
            outs=places,
            scratch=[pltpu.SemaphoreType.DMA((2 * len(steps),))],
        )

    place = pltpu.HBM(shape, BF)
    one, three, own, two = cut((1, 3, 0, 2), [place] * peers, "aaaa")
    swapped = [own]
    for far, block in ((1, one), (2, two), (3, three)):
        swapped.append(shifted(block, "tp_1", far))
    return swapped


def both_halves(
    queries,
    keys,
    values,
    gates,
    log_decay,
    out_weight,
    moe_rows,
    moe_gain,
    routes,
    route_weights,
    gate_proj,
    up_proj,
    down_proj,
):
    experts = lax.axis_size(EP)
    members = lax.axis_size(TP)
    tokens = moe_rows.shape[0]
    positions = queries.shape[0]
    lane = lax.axis_index("tp_1")
    room = 2 * tokens // experts
    count = experts * room
    rows_y = lax.axis_size("tp_0")
    peers = lax.axis_size("tp_1")
    units = gate_proj.shape[2]
    tall = 2 * count + positions
    send, slots = dispatch(moe_rows, moe_gain, routes, experts, lax.axis_index(TP).reshape(1))
    weights = exchanged_weights(down_proj, out_weight, lane)
    arrived = lax.all_to_all(send, EP, 0, 0, tiled=True)
    spread = call(
        spread_body,
        pltpu.HBM((members, count, HEAD), BF),
        arrived.reshape(count, HEAD),
        kinds="v",
        outs="a",
        scratch=[pltpu.SemaphoreType.DMA((members,))],
    )
    rows = lax.all_to_all(spread, TP, 0, 0, tiled=True)
    head_out = retention_heads(queries, keys, values, gates, log_decay)
    width = gate_proj.shape[1]
    mixed = call(
        hidden_body,
        pltpu.HBM((rows_y, tall, HEAD), BF),
        rows,
        head_out,
        gate_proj,
        up_proj,
        kinds="vvaa",
        outs="a",
        scratch=[
            pltpu.VMEM((width, units), BF),
            pltpu.VMEM((width, units), BF),
            pltpu.VMEM((tall, HEAD), BF),
            pltpu.SemaphoreType.DMA((2, 8)),
            pltpu.SemaphoreType.DMA((rows_y,)),
        ],
    )
    got = lax.all_to_all(mixed, "tp_0", 0, 0, tiled=True)
    partial = call(
        project_body,
        onchip((peers, count + positions, HEAD), BF),
        lane.reshape(1),
        got,
        *weights,
        kinds="svhhhh",
    )
    pieces = lax.all_to_all(partial, "tp_1", 0, 0, tiled=True)
    summed, mixer_out = call(
        add_body,
        [onchip((experts, room, HEAD), BF), shaped((positions, HEAD), BF)],
        pieces,
        kinds="v",
        outs="vh",
    )
    back = lax.all_to_all(summed, EP, 0, 0, tiled=True)
    columns, scales = lax.optimization_barrier((slots.T, route_weights))
    moe_out = call(
        combine_body, shaped((tokens, HEAD), BF), back, columns, scales, kinds="vvv", outs="h"
    )
    return (mixer_out, moe_out)


def solution(mesh):
    torus = Mesh(mesh.devices.reshape(8, 2, 2, 4, 4), ("ep_0", "ep_1", "ep_2", "tp_0", "tp_1"))
    return jax.shard_map(
        both_halves,
        mesh=torus,
        in_specs=(
            P(EP, TP),
            P(EP, TP),
            P(EP, TP),
            P(EP, TP),
            P(EP, TP),
            P(None, TP),
            P(EP, None),
            P(),
            P(EP, None),
            P(EP, None),
            P(EP, None, TP),
            P(EP, None, TP),
            P(EP, None, TP),
        ),
        out_specs=(P(EP, TP), P(EP, TP)),
        check_vma=False,
    )
```

```python
import functools

import jax
import jax.numpy as jnp
from jax import lax
from jax.experimental import pallas as pl
from jax.experimental.pallas import tpu as pltpu
from jax.sharding import Mesh
from jax.sharding import PartitionSpec as P

BLOCK = 128
HEAD = 128
EP = ("ep_0", "ep_1", "ep_2")
TP = ("tp_0", "tp_1")
BF = jnp.bfloat16
F32 = jnp.float32
HIGH = lax.Precision.HIGHEST
PAY = HEAD + 16
LIMIT = 12 * 1024 * 1024


def dot(a, b, dims=((1,), (0,)), precision=None):
    return lax.dot_general(a, b, (dims, ((), ())), precision=precision, preferred_element_type=F32)


def shaped(shape, dtype):
    return jax.ShapeDtypeStruct(shape, dtype)


def onchip(shape, dtype):
    return pltpu.VMEM(shape, dtype)


def call(body, out_shape, *args, kinds, outs="v", scratch=()):
    places = {
        "s": pl.BlockSpec(memory_space=pltpu.SMEM),
        "v": pl.BlockSpec(memory_space=pltpu.VMEM),
        "h": pl.BlockSpec(),
        "p": pl.BlockSpec(),
        "a": pl.BlockSpec(memory_space=pltpu.HBM),
    }
    held = [
        pltpu.with_memory_space_constraint(arg, {"v": pltpu.VMEM}.get(kind, pltpu.HBM))
        if kind in "vpa"
        else arg
        for arg, kind in zip(args, kinds, strict=True)
    ]
    single = not isinstance(out_shape, (list, tuple))
    out_specs = [places[kind] for kind in outs]
    return pl.pallas_call(
        body,
        in_specs=[places[kind] for kind in kinds],
        out_specs=out_specs[0] if single else out_specs,
        out_shape=out_shape,
        scratch_shapes=list(scratch),
        compiler_params=pltpu.CompilerParams(vmem_limit_bytes=LIMIT),
    )(*held)


def route_body(turn, routes_far, gain_far, source, send, slots, routes, gain, rows, sems, extra):
    tokens = rows.shape[0]
    experts = send.shape[0]
    room = send.shape[1]
    chunks = sems.shape[0]
    tall = tokens // chunks
    copies = [
        pltpu.make_async_copy(
            source.at[pl.ds(k * tall, tall)], rows.at[pl.ds(k * tall, tall)], sems.at[k]
        )
        for k in range(chunks)
    ]
    small = pltpu.make_async_copy(routes_far, routes, extra.at[0])
    scales = pltpu.make_async_copy(gain_far, gain, extra.at[1])
    small.start()
    for copy in copies:
        copy.start()
    scales.start()
    small.wait()
    first = routes[0:1, :]
    second = routes[1:2, :]
    expert = lax.broadcasted_iota(jnp.int32, (experts, tokens), 0)
    is_first = expert == first
    is_second = expert == second
    named = jnp.where(is_first | is_second, 1.0, 0.0).astype(BF)
    earlier = lax.broadcasted_iota(jnp.int32, (tokens, tokens), 0) < lax.broadcasted_iota(
        jnp.int32, (tokens, tokens), 1
    )
    rank = dot(named, jnp.where(earlier, 1.0, 0.0).astype(BF)).astype(jnp.int32)
    slot_a = first * room + jnp.sum(jnp.where(is_first, rank, 0), axis=0, keepdims=True)
    slot_b = second * room + jnp.sum(jnp.where(is_second, rank, 0), axis=0, keepdims=True)
    slots[0:1, :] = slot_a
    slots[1:2, :] = slot_b
    place = lax.broadcasted_iota(jnp.int32, (experts * room, tokens), 0)
    chosen = jnp.where((place == slot_a) | (place == slot_b), 1.0, 0.0).astype(BF)
    scales.wait()
    which = lax.broadcasted_iota(jnp.int32, gain.shape, 0) == turn[0]
    scale = jnp.sum(jnp.where(which, gain[...].astype(F32), 0.0), axis=0, keepdims=True)
    at = pl.multiple_of(turn[0] * HEAD, HEAD)
    parts = []
    for k, copy in enumerate(copies):
        copy.wait()
        wide = rows[k * tall : (k + 1) * tall, :].astype(F32)
        power = jnp.mean(wide * wide, axis=-1, keepdims=True)
        part = rows[k * tall : (k + 1) * tall, pl.ds(at, HEAD)].astype(F32)
        parts.append((part * lax.rsqrt(power + 1e-06) * scale).astype(BF))
    normed = jnp.concatenate(parts, axis=0)
    send[...] = dot(chosen, normed).astype(BF).reshape(experts, room, HEAD)


def dispatch(moe_rows, moe_gain, routes, experts, turn):
    tokens, width = moe_rows.shape
    room = 2 * tokens // experts
    return call(
        route_body,
        [onchip((experts, room, HEAD), BF), onchip((2, tokens), jnp.int32)],
        turn,
        routes.T,
        moe_gain.reshape(width // HEAD, HEAD),
        moe_rows,
        kinds="saaa",
        outs="vv",
        scratch=[
            pltpu.VMEM((2, tokens), jnp.int32),
            pltpu.VMEM((width // HEAD, HEAD), BF),
            pltpu.VMEM((tokens, width), BF),
            pltpu.SemaphoreType.DMA((8,)),
            pltpu.SemaphoreType.DMA((2,)),
        ],
    )


def spread_body(rows, out, sems):
    copies = [pltpu.make_async_copy(rows, out.at[k], sems.at[k]) for k in range(out.shape[0])]
    for copy in copies:
        copy.start()
    for copy in copies:
        copy.wait()


def hidden_body(rows, heads, w_gate, w_up, out, near_gate, near_up, near, sems, ends):
    parts, count, _ = rows.shape
    copied = out.shape[0]
    chunks = sems.shape[1]
    tall = w_gate.shape[1] // chunks
    copies = []
    for k in range(chunks):
        span = pl.ds(k * tall, tall)
        copies.append(
            (
                pltpu.make_async_copy(w_gate.at[0, span], near_gate.at[span], sems.at[0, k]),
                pltpu.make_async_copy(w_up.at[0, span], near_up.at[span], sems.at[1, k]),
            )
        )
    for kind in range(2):
        for pair in copies:
            pair[kind].start()
    near[2 * count :, :] = heads[...]
    per = parts // chunks
    half = count // 2
    final = []
    for side in range(2):
        span = slice(side * half, (side + 1) * half)
        sums = []
        for kind, near_w in ((0, near_gate), (1, near_up)):
            total = jnp.zeros((half, w_gate.shape[2]), F32)
            for k in range(chunks):
                if side == 0:
                    copies[k][kind].wait()
                left = jnp.concatenate([rows[k * per + j, span, :] for j in range(per)], axis=1)
                total += dot(left, near_w[k * tall : (k + 1) * tall, :])
            sums.append(total)
        gate, up = sums
        hidden = (gate / (1.0 + jnp.exp(-gate)) * up).astype(BF)
        for part in range(2):
            at = part * count + side * half
            near[at : at + half, :] = hidden[:, part * HEAD : (part + 1) * HEAD]
            for k in range(copied):
                here = pl.ds(at, half)
                copy = pltpu.make_async_copy(
                    near.at[here], out.at[k, here], ends.at[k, 2 * side + part]
                )
                copy.start()
                final.append(copy)
        if side == 0:
            here = pl.ds(2 * count, heads.shape[0])
            for k in range(copied):
                copy = pltpu.make_async_copy(near.at[here], out.at[k, here], ends.at[k, 4])
                copy.start()
                final.append(copy)
    for copy in final:
        copy.wait()


def project_body(lane, got, down, weight, w_1, w_2, w_3, out, own, sems):
    peers = got.shape[0]
    positions = got.shape[1] // 5
    count = 2 * positions
    units = 2 * HEAD
    copies = [
        pltpu.make_async_copy(down.at[:, lane[0]], own.at[:, 0:units], sems.at[0]),
        pltpu.make_async_copy(weight.at[:, lane[0]], own.at[:, units:], sems.at[1]),
    ]
    for copy in copies:
        copy.start()
    left = [
        jnp.concatenate([got[k, 0:count, :], got[k, count : 2 * count, :]], axis=1)
        for k in range(peers)
    ]
    for (one, two), steps in (((w_2, w_3), (2, 3)), ((own, w_1), (0, 1))):
        if steps[0] == 0:
            for copy in copies:
                copy.wait()
        expert = jnp.zeros((count, 2 * HEAD), F32)
        mixer = jnp.zeros((positions, 2 * HEAD), F32)
        for k in range(peers):
            both = jnp.concatenate([one[k], two[k]], axis=1)
            expert += dot(left[k], both[0:units])
            mixer += dot(got[k, 2 * count :, :], both[units:])
        for which, step in enumerate(steps):
            at = (lane[0] + peers - step) % peers
            cols = slice(which * HEAD, which * HEAD + HEAD)
            out[pl.ds(at, 1), 0:count, :] = expert[:, cols].astype(BF)[None]
            out[pl.ds(at, 1), count:, :] = mixer[:, cols].astype(BF)[None]


def add_body(parts, experts, mixer):
    total = parts[0].astype(F32)
    for k in range(1, parts.shape[0]):
        total += parts[k].astype(F32)
    count = experts.shape[0] * experts.shape[1]
    experts[...] = total[0:count].astype(BF).reshape(experts.shape)
    mixer[...] = total[count:].astype(BF)


def combine_body(back, slots, weights, out):
    experts, room, _ = back.shape
    rows = back[...].reshape(experts * room, HEAD)
    tokens = slots.shape[0]
    place = lax.broadcasted_iota(jnp.int32, (tokens, experts * room), 1)
    total = jnp.zeros((tokens, HEAD), F32)
    for k in range(2):
        chosen = jnp.where(place == slots[:, k : k + 1], 1.0, 0.0).astype(BF)
        total += dot(chosen, rows) * weights[:, k : k + 1]
    out[...] = total.astype(BF)


def local_body(q, k, v, decay, cosine, sine, base, q_decayed, pay):
    count = q.shape[0]
    blocks = count // BLOCK
    cos = cosine[...]
    sin = sine[...]
    rows = lax.broadcasted_iota(jnp.int32, (BLOCK, BLOCK), 0)
    cols = lax.broadcasted_iota(jnp.int32, (BLOCK, BLOCK), 1)
    causal = rows >= cols
    upper = jnp.where(rows <= cols, 1.0, 0.0)
    lower = jnp.where(causal, 1.0, 0.0)

    def turned(x, factor):
        wide = x.astype(F32)
        swapped = pltpu.roll(wide, HEAD // 2, 1)
        return ((wide * cos + swapped * sin) * factor).astype(BF)

    q_all = turned(q[...], 1.0)
    k_all = turned(k[...], HEAD ** (-0.5))
    carried = jnp.zeros((HEAD, HEAD), F32)
    leading = jnp.zeros((1, HEAD), F32)
    for n in range(blocks):
        span = slice(n * BLOCK, n * BLOCK + BLOCK)
        q_b, k_b, v_b = q_all[span], k_all[span], v[span, :]
        here = jnp.broadcast_to(decay[n : n + 1, :], (BLOCK, BLOCK))
        cum_i = dot(lower, here, ((1,), (1,)), HIGH)
        cum_j = dot(here, upper, precision=HIGH)
        weights = jnp.where(causal, jnp.exp(jnp.where(causal, cum_i - cum_j, 0.0)), 0.0)
        scores = dot(q_b, k_b, ((1,), (1,)))
        inside = dot((scores * weights).astype(BF), v_b)
        q_f = q_b.astype(F32)
        q_d = q_f * jnp.exp(cum_i)
        if n:
            inside += dot(q_d, carried, precision=HIGH)
        base[span, :] = inside
        q_decayed[span, :] = q_f * jnp.exp(cum_i + leading)
        ending = cum_i[BLOCK - 1 : BLOCK, :]
        k_scaled = k_b.astype(F32) * jnp.exp(ending - cum_i)
        update = dot(k_scaled, v_b.astype(F32), ((0,), (0,)), HIGH)
        carried = jnp.exp(ending) * carried + update
        leading = leading + ending
    packed(pay, carried, leading)


def packed(pay, state, total):
    pay[0 : state.shape[0], :] = state.astype(BF)
    high = total.astype(BF)
    rest = total - high.astype(F32)
    middle = rest.astype(BF)
    low = (rest - middle.astype(F32)).astype(BF)
    row = lax.broadcasted_iota(jnp.int32, (16, HEAD), 0)
    three = jnp.where(
        row == 0,
        high.astype(F32),
        jnp.where(row == 1, middle.astype(F32), jnp.where(row == 2, low.astype(F32), 0.0)),
    )
    pay[state.shape[0] :, :] = three.astype(BF)


def unpacked(pay):
    rows = pay.shape[0] - 16
    tail = pay[rows:, :].astype(F32)
    return pay[0:rows, :].astype(F32), tail[0:1] + tail[1:2] + tail[2:3]


def quad_body(core, near, pay):
    state, decay = unpacked(near.at[0])
    for k in range(1, near.shape[0]):
        later, later_decay = unpacked(near.at[k])
        state = later + jnp.exp(later_decay) * state
        decay = decay + later_decay
    half = HEAD // 2
    mine = jnp.where(core[0] == 0, state[0:half], state[half:])
    packed(pay, mine, decay)


def head_body(place, group, far, near, base, q_decayed, gates, out):
    entering = jnp.zeros((HEAD, HEAD), F32)
    for k in range(far.shape[0] // 2):
        upper, decay = unpacked(far.at[2 * k])
        lower, _ = unpacked(far.at[2 * k + 1])
        state = jnp.concatenate([upper, lower], axis=0)
        entering = jnp.where(k < group[0], jnp.exp(decay) * entering + state, entering)
    for k in range(near.shape[0] - 1):
        state, decay = unpacked(near.at[k])
        entering = jnp.where(k < place[0], jnp.exp(decay) * entering + state, entering)
    retained = base[...] + dot(q_decayed[...], entering, precision=HIGH)
    power = jnp.mean(retained * retained, axis=-1, keepdims=True)
    gate = gates[...].astype(F32)
    out[...] = (retained * lax.rsqrt(power + 1e-05) * (gate / (1.0 + jnp.exp(-gate)))).astype(BF)


def retention_heads(queries, keys, values, gates, log_decay):
    count = queries.shape[0]
    positions = (lax.axis_index(EP) * count + jnp.arange(count, dtype=jnp.int32)).astype(F32)
    half = HEAD // 2
    inverse = 10000.0 ** (-jnp.arange(half, dtype=F32) / half)
    angles = positions[:, None] * jnp.concatenate([inverse, inverse])[None, :]
    cosine = jnp.cos(angles)
    sine = jnp.sin(angles) * jnp.where(jnp.arange(HEAD) < half, -1.0, 1.0)[None, :]
    flat = pltpu.HBM((count, HEAD), F32)
    base, q_decayed, pay = call(
        local_body,
        [flat, flat, onchip((PAY, HEAD), BF)],
        queries,
        keys,
        values,
        log_decay.reshape(count // BLOCK, BLOCK),
        cosine,
        sine,
        kinds="ppppvv",
        outs="hhv",
    )
    place = lax.axis_index(("ep_1", "ep_2")).reshape(1)
    near = lax.all_gather(pay, ("ep_1", "ep_2"))
    pay = call(
        quad_body,
        onchip((PAY - HEAD // 2, HEAD), BF),
        lax.axis_index("ep_2").reshape(1),
        near,
        kinds="sv",
    )
    far = lax.all_gather(pay, ("ep_0", "ep_2"))
    return call(
        head_body,
        shaped((count, HEAD), BF),
        place,
        lax.axis_index("ep_0").reshape(1),
        far,
        near,
        base,
        q_decayed,
        gates,
        kinds="sshhpph",
        outs="h",
    )


def cut_body(far, lane, down, heads, *rest):
    peers = down.shape[1]
    outs, sems = rest[: len(far)], rest[len(far)]
    units = down.shape[2]
    copies = []
    for k, step in enumerate(far):
        at = (lane[0] + step) % peers
        copies.append(
            pltpu.make_async_copy(down.at[:, at], outs[k].at[:, 0:units], sems.at[2 * k])
        )
        copies.append(
            pltpu.make_async_copy(heads.at[:, at], outs[k].at[:, units:], sems.at[2 * k + 1])
        )
    for copy in copies:
        copy.start()
    for copy in copies:
        copy.wait()


def shifted(array, axis, far):
    peers = lax.axis_size(axis)
    return lax.ppermute(array, axis, [(k, (k + far) % peers) for k in range(peers)])


def exchanged_weights(down_proj, out_weight, lane):
    peers = lax.axis_size("tp_1")
    rows = lax.axis_size("tp_0")
    down = down_proj.reshape(rows, peers, -1, HEAD)
    heads = out_weight.reshape(rows, peers, -1, HEAD)
    shape = (rows, down.shape[2] + heads.shape[2], HEAD)

    def cut(steps, outs, places):
        return call(
            functools.partial(cut_body, steps),
            outs,
            lane.reshape(1),
            down,
            heads,
            kinds="saa",
            outs=places,
            scratch=[pltpu.SemaphoreType.DMA((2 * len(steps),))],
        )

    place = onchip(shape, BF)
    one, three = cut((1, 3), [place] * 2, "vv")
    (two,) = cut((2,), [place], "v")
    swapped = []
    for far, block in ((1, one), (2, two), (3, three)):
        swapped.append(shifted(block, "tp_1", far))
    return [down, heads, *swapped]


def both_halves(
    queries,
    keys,
    values,
    gates,
    log_decay,
    out_weight,
    moe_rows,
    moe_gain,
    routes,
    route_weights,
    gate_proj,
    up_proj,
    down_proj,
):
    experts = lax.axis_size(EP)
    members = lax.axis_size(TP)
    tokens = moe_rows.shape[0]
    positions = queries.shape[0]
    lane = lax.axis_index("tp_1")
    room = 2 * tokens // experts
    count = experts * room
    rows_y = lax.axis_size("tp_0")
    peers = lax.axis_size("tp_1")
    units = gate_proj.shape[2]
    tall = 2 * count + positions
    send, slots = dispatch(moe_rows, moe_gain, routes, experts, lax.axis_index(TP).reshape(1))
    weights = exchanged_weights(down_proj, out_weight, lane)
    arrived = lax.all_to_all(send, EP, 0, 0, tiled=True)
    spread = call(
        spread_body,
        pltpu.HBM((members, count, HEAD), BF),
        arrived.reshape(count, HEAD),
        kinds="v",
        outs="a",
        scratch=[pltpu.SemaphoreType.DMA((members,))],
    )
    rows = lax.all_to_all(spread, TP, 0, 0, tiled=True)
    head_out = retention_heads(queries, keys, values, gates, log_decay)
    width = gate_proj.shape[1]
    mixed = call(
        hidden_body,
        pltpu.HBM((rows_y, tall, HEAD), BF),
        rows,
        head_out,
        gate_proj,
        up_proj,
        kinds="vvaa",
        outs="a",
        scratch=[
            pltpu.VMEM((width, units), BF),
            pltpu.VMEM((width, units), BF),
            pltpu.VMEM((tall, HEAD), BF),
            pltpu.SemaphoreType.DMA((2, 8)),
            pltpu.SemaphoreType.DMA((rows_y, 5)),
        ],
    )
    got = lax.all_to_all(mixed, "tp_0", 0, 0, tiled=True)
    partial = call(
        project_body,
        onchip((peers, count + positions, HEAD), BF),
        lane.reshape(1),
        got,
        *weights,
        kinds="svaahhh",
        scratch=[pltpu.VMEM(weights[-1].shape, BF), pltpu.SemaphoreType.DMA((2,))],
    )
    pieces = lax.all_to_all(partial, "tp_1", 0, 0, tiled=True)
    summed, mixer_out = call(
        add_body,
        [onchip((experts, room, HEAD), BF), shaped((positions, HEAD), BF)],
        pieces,
        kinds="v",
        outs="vh",
    )
    back = lax.all_to_all(summed, EP, 0, 0, tiled=True)
    columns, scales = lax.optimization_barrier((slots.T, route_weights))
    moe_out = call(
        combine_body, shaped((tokens, HEAD), BF), back, columns, scales, kinds="vvv", outs="h"
    )
    return (mixer_out, moe_out)


def solution(mesh):
    torus = Mesh(mesh.devices.reshape(8, 2, 2, 4, 4), ("ep_0", "ep_1", "ep_2", "tp_0", "tp_1"))
    return jax.shard_map(
        both_halves,
        mesh=torus,
        in_specs=(
            P(EP, TP),
            P(EP, TP),
            P(EP, TP),
            P(EP, TP),
            P(EP, TP),
            P(None, TP),
            P(EP, None),
            P(),
            P(EP, None),
            P(EP, None),
            P(EP, None, TP),
            P(EP, None, TP),
            P(EP, None, TP),
        ),
        out_specs=(P(EP, TP), P(EP, TP)),
        check_vma=False,
    )
```

```python
import functools

import jax
import jax.numpy as jnp
from jax import lax
from jax.experimental import pallas as pl
from jax.experimental.pallas import tpu as pltpu
from jax.sharding import Mesh
from jax.sharding import PartitionSpec as P

BLOCK = 128
HEAD = 128
EP = ("ep_0", "ep_1", "ep_2")
TP = ("tp_0", "tp_1")
BF = jnp.bfloat16
F32 = jnp.float32
HIGH = lax.Precision.HIGHEST
PAY = HEAD + 16
LIMIT = 12 * 1024 * 1024


def dot(a, b, dims=((1,), (0,)), precision=None):
    return lax.dot_general(a, b, (dims, ((), ())), precision=precision, preferred_element_type=F32)


def shaped(shape, dtype):
    return jax.ShapeDtypeStruct(shape, dtype)


def onchip(shape, dtype):
    return pltpu.VMEM(shape, dtype)


def call(body, out_shape, *args, kinds, outs="v", scratch=()):
    places = {
        "s": pl.BlockSpec(memory_space=pltpu.SMEM),
        "v": pl.BlockSpec(memory_space=pltpu.VMEM),
        "h": pl.BlockSpec(),
        "p": pl.BlockSpec(),
        "a": pl.BlockSpec(memory_space=pltpu.HBM),
    }
    held = [
        pltpu.with_memory_space_constraint(arg, {"v": pltpu.VMEM}.get(kind, pltpu.HBM))
        if kind in "vpa"
        else arg
        for arg, kind in zip(args, kinds, strict=True)
    ]
    single = not isinstance(out_shape, (list, tuple))
    out_specs = [places[kind] for kind in outs]
    return pl.pallas_call(
        body,
        in_specs=[places[kind] for kind in kinds],
        out_specs=out_specs[0] if single else out_specs,
        out_shape=out_shape,
        scratch_shapes=list(scratch),
        compiler_params=pltpu.CompilerParams(vmem_limit_bytes=LIMIT),
    )(*held)


def route_body(turn, routes_far, gain_far, source, send, slots, routes, gain, rows, sems, extra):
    tokens = rows.shape[0]
    experts = send.shape[0]
    room = send.shape[1]
    chunks = sems.shape[0]
    tall = tokens // chunks
    copies = [
        pltpu.make_async_copy(
            source.at[pl.ds(k * tall, tall)], rows.at[pl.ds(k * tall, tall)], sems.at[k]
        )
        for k in range(chunks)
    ]
    small = pltpu.make_async_copy(routes_far, routes, extra.at[0])
    scales = pltpu.make_async_copy(gain_far, gain, extra.at[1])
    small.start()
    for copy in copies:
        copy.start()
    scales.start()
    small.wait()
    first = routes[0:1, :]
    second = routes[1:2, :]
    expert = lax.broadcasted_iota(jnp.int32, (experts, tokens), 0)
    is_first = expert == first
    is_second = expert == second
    named = jnp.where(is_first | is_second, 1.0, 0.0).astype(BF)
    earlier = lax.broadcasted_iota(jnp.int32, (tokens, tokens), 0) < lax.broadcasted_iota(
        jnp.int32, (tokens, tokens), 1
    )
    rank = dot(named, jnp.where(earlier, 1.0, 0.0).astype(BF)).astype(jnp.int32)
    slot_a = first * room + jnp.sum(jnp.where(is_first, rank, 0), axis=0, keepdims=True)
    slot_b = second * room + jnp.sum(jnp.where(is_second, rank, 0), axis=0, keepdims=True)
    slots[0:1, :] = slot_a
    slots[1:2, :] = slot_b
    place = lax.broadcasted_iota(jnp.int32, (experts * room, tokens), 0)
    chosen = jnp.where((place == slot_a) | (place == slot_b), 1.0, 0.0).astype(BF)
    scales.wait()
    which = lax.broadcasted_iota(jnp.int32, gain.shape, 0) == turn[0]
    scale = jnp.sum(jnp.where(which, gain[...].astype(F32), 0.0), axis=0, keepdims=True)
    at = pl.multiple_of(turn[0] * HEAD, HEAD)
    parts = []
    for k, copy in enumerate(copies):
        copy.wait()
        wide = rows[k * tall : (k + 1) * tall, :].astype(F32)
        power = jnp.mean(wide * wide, axis=-1, keepdims=True)
        part = rows[k * tall : (k + 1) * tall, pl.ds(at, HEAD)].astype(F32)
        parts.append((part * lax.rsqrt(power + 1e-06) * scale).astype(BF))
    normed = jnp.concatenate(parts, axis=0)
    send[...] = dot(chosen, normed).astype(BF).reshape(experts, room, HEAD)


def dispatch(moe_rows, moe_gain, routes, experts, turn):
    tokens, width = moe_rows.shape
    room = 2 * tokens // experts
    return call(
        route_body,
        [onchip((experts, room, HEAD), BF), onchip((2, tokens), jnp.int32)],
        turn,
        routes.T,
        moe_gain.reshape(width // HEAD, HEAD),
        moe_rows,
        kinds="saaa",
        outs="vv",
        scratch=[
            pltpu.VMEM((2, tokens), jnp.int32),
            pltpu.VMEM((width // HEAD, HEAD), BF),
            pltpu.VMEM((tokens, width), BF),
            pltpu.SemaphoreType.DMA((8,)),
            pltpu.SemaphoreType.DMA((2,)),
        ],
    )


def spread_body(rows, out, sems):
    copies = [pltpu.make_async_copy(rows, out.at[k], sems.at[k]) for k in range(out.shape[0])]
    for copy in copies:
        copy.start()
    for copy in copies:
        copy.wait()


def hidden_body(rows, heads, w_gate, w_up, out, near_gate, near_up, near, sems, ends):
    parts, count, _ = rows.shape
    copied = out.shape[0]
    chunks = sems.shape[1]
    tall = w_gate.shape[1] // chunks
    copies = []
    for k in range(chunks):
        span = pl.ds(k * tall, tall)
        copies.append(
            (
                pltpu.make_async_copy(w_gate.at[0, span], near_gate.at[span], sems.at[0, k]),
                pltpu.make_async_copy(w_up.at[0, span], near_up.at[span], sems.at[1, k]),
            )
        )
    for kind in range(2):
        for pair in copies:
            pair[kind].start()
    near[2 * count :, :] = heads[...]
    per = parts // chunks
    half = count // 2
    final = []
    for side in range(2):
        span = slice(side * half, (side + 1) * half)
        sums = []
        for kind, near_w in ((0, near_gate), (1, near_up)):
            total = jnp.zeros((half, w_gate.shape[2]), F32)
            for k in range(chunks):
                if side == 0:
                    copies[k][kind].wait()
                left = jnp.concatenate([rows[k * per + j, span, :] for j in range(per)], axis=1)
                total += dot(left, near_w[k * tall : (k + 1) * tall, :])
            sums.append(total)
        gate, up = sums
        hidden = (gate / (1.0 + jnp.exp(-gate)) * up).astype(BF)
        for part in range(2):
            at = part * count + side * half
            near[at : at + half, :] = hidden[:, part * HEAD : (part + 1) * HEAD]
            for k in range(copied):
                here = pl.ds(at, half)
                copy = pltpu.make_async_copy(
                    near.at[here], out.at[k, here], ends.at[k, 2 * side + part]
                )
                copy.start()
                final.append(copy)
        if side == 0:
            here = pl.ds(2 * count, heads.shape[0])
            for k in range(copied):
                copy = pltpu.make_async_copy(near.at[here], out.at[k, here], ends.at[k, 4])
                copy.start()
                final.append(copy)
    for copy in final:
        copy.wait()


def project_body(lane, got, down, weight, w_1, w_2, w_3, out, m_0, m_1, m_2, m_3, own, sems):
    peers = got.shape[0]
    positions = got.shape[1] // 5
    count = 2 * positions
    units = 2 * HEAD
    copies = [
        pltpu.make_async_copy(down.at[:, lane[0]], own.at[:, 0:units], sems.at[0]),
        pltpu.make_async_copy(weight.at[:, lane[0]], own.at[:, units:], sems.at[1]),
    ]
    for copy in copies:
        copy.start()
    left = [
        jnp.concatenate([got[k, 0:count, :], got[k, count : 2 * count, :]], axis=1)
        for k in range(peers)
    ]
    mixes = (m_0, m_1, m_2, m_3)
    for (one, two), steps in (((w_2, w_3), (2, 3)), ((own, w_1), (0, 1))):
        if steps[0] == 0:
            for copy in copies:
                copy.wait()
        expert = jnp.zeros((count, 2 * HEAD), F32)
        mixer = jnp.zeros((positions, 2 * HEAD), F32)
        for k in range(peers):
            both = jnp.concatenate([one[k], two[k]], axis=1)
            expert += dot(left[k], both[0:units])
            mixer += dot(got[k, 2 * count :, :], both[units:])
        for which, step in enumerate(steps):
            at = (lane[0] + peers - step) % peers
            cols = slice(which * HEAD, which * HEAD + HEAD)
            out[pl.ds(at, 1)] = expert[:, cols].astype(BF)[None]
            mixes[step][...] = mixer[:, cols].astype(BF)


def add_body(parts, out):
    total = parts[0].astype(F32)
    for k in range(1, parts.shape[0]):
        total += parts[k].astype(F32)
    out[...] = total.astype(BF).reshape(out.shape)


def add_four_body(p_0, p_1, p_2, p_3, out):
    out[...] = (
        (p_0[...].astype(F32) + p_1[...].astype(F32))
        + (p_2[...].astype(F32) + p_3[...].astype(F32))
    ).astype(BF)


def combine_body(back, slots, weights, out):
    experts, room, _ = back.shape
    rows = back[...].reshape(experts * room, HEAD)
    tokens = slots.shape[0]
    place = lax.broadcasted_iota(jnp.int32, (tokens, experts * room), 1)
    total = jnp.zeros((tokens, HEAD), F32)
    for k in range(2):
        chosen = jnp.where(place == slots[:, k : k + 1], 1.0, 0.0).astype(BF)
        total += dot(chosen, rows) * weights[:, k : k + 1]
    out[...] = total.astype(BF)


def local_body(q, k, v, decay, cosine, sine, base, q_decayed, pay):
    count = q.shape[0]
    blocks = count // BLOCK
    cos = cosine[...]
    sin = sine[...]
    rows = lax.broadcasted_iota(jnp.int32, (BLOCK, BLOCK), 0)
    cols = lax.broadcasted_iota(jnp.int32, (BLOCK, BLOCK), 1)
    causal = rows >= cols
    upper = jnp.where(rows <= cols, 1.0, 0.0)
    lower = jnp.where(causal, 1.0, 0.0)

    def turned(x, factor):
        wide = x.astype(F32)
        swapped = pltpu.roll(wide, HEAD // 2, 1)
        return ((wide * cos + swapped * sin) * factor).astype(BF)

    q_all = turned(q[...], 1.0)
    k_all = turned(k[...], HEAD ** (-0.5))
    carried = jnp.zeros((HEAD, HEAD), F32)
    leading = jnp.zeros((1, HEAD), F32)
    for n in range(blocks):
        span = slice(n * BLOCK, n * BLOCK + BLOCK)
        q_b, k_b, v_b = q_all[span], k_all[span], v[span, :]
        here = jnp.broadcast_to(decay[n : n + 1, :], (BLOCK, BLOCK))
        cum_i = dot(lower, here, ((1,), (1,)), HIGH)
        cum_j = dot(here, upper, precision=HIGH)
        weights = jnp.where(causal, jnp.exp(jnp.where(causal, cum_i - cum_j, 0.0)), 0.0)
        scores = dot(q_b, k_b, ((1,), (1,)))
        inside = dot((scores * weights).astype(BF), v_b)
        q_f = q_b.astype(F32)
        q_d = q_f * jnp.exp(cum_i)
        if n:
            inside += dot(q_d, carried, precision=HIGH)
        base[span, :] = inside
        q_decayed[span, :] = q_f * jnp.exp(cum_i + leading)
        ending = cum_i[BLOCK - 1 : BLOCK, :]
        k_scaled = k_b.astype(F32) * jnp.exp(ending - cum_i)
        update = dot(k_scaled, v_b.astype(F32), ((0,), (0,)), HIGH)
        carried = jnp.exp(ending) * carried + update
        leading = leading + ending
    packed(pay, carried, leading)


def packed(pay, state, total):
    pay[0 : state.shape[0], :] = state.astype(BF)
    high = total.astype(BF)
    rest = total - high.astype(F32)
    middle = rest.astype(BF)
    low = (rest - middle.astype(F32)).astype(BF)
    row = lax.broadcasted_iota(jnp.int32, (16, HEAD), 0)
    three = jnp.where(
        row == 0,
        high.astype(F32),
        jnp.where(row == 1, middle.astype(F32), jnp.where(row == 2, low.astype(F32), 0.0)),
    )
    pay[state.shape[0] :, :] = three.astype(BF)


def unpacked(pay):
    rows = pay.shape[0] - 16
    tail = pay[rows:, :].astype(F32)
    return pay[0:rows, :].astype(F32), tail[0:1] + tail[1:2] + tail[2:3]


def quad_body(core, near, pay):
    state, decay = unpacked(near.at[0])
    for k in range(1, near.shape[0]):
        later, later_decay = unpacked(near.at[k])
        state = later + jnp.exp(later_decay) * state
        decay = decay + later_decay
    half = HEAD // 2
    mine = jnp.where(core[0] == 0, state[0:half], state[half:])
    packed(pay, mine, decay)


def head_body(
    place, group, lane, far, near, base, q_decayed, gates, down, weight, out, b_1, b_3, here, sems
):
    peers = down.shape[1]
    units = down.shape[2]
    loads, stores = [], []
    for k, (step, block) in enumerate(((1, b_1), (3, b_3))):
        at = (lane[0] + step) % peers
        loads.append(
            (
                pltpu.make_async_copy(down.at[:, at], here.at[k, :, 0:units], sems.at[3 * k]),
                pltpu.make_async_copy(weight.at[:, at], here.at[k, :, units:], sems.at[3 * k + 1]),
            )
        )
        stores.append(pltpu.make_async_copy(here.at[k], block, sems.at[3 * k + 2]))
    for one, two in loads:
        one.start()
        two.start()
    entering = jnp.zeros((HEAD, HEAD), F32)
    for k in range(far.shape[0] // 2):
        upper, decay = unpacked(far.at[2 * k])
        lower, _ = unpacked(far.at[2 * k + 1])
        state = jnp.concatenate([upper, lower], axis=0)
        entering = jnp.where(k < group[0], jnp.exp(decay) * entering + state, entering)
    for k in range(near.shape[0] - 1):
        state, decay = unpacked(near.at[k])
        entering = jnp.where(k < place[0], jnp.exp(decay) * entering + state, entering)
    for (one, two), store in zip(loads, stores, strict=True):
        one.wait()
        two.wait()
        store.start()
    retained = base[...] + dot(q_decayed[...], entering, precision=HIGH)
    power = jnp.mean(retained * retained, axis=-1, keepdims=True)
    gate = gates[...].astype(F32)
    out[...] = (retained * lax.rsqrt(power + 1e-05) * (gate / (1.0 + jnp.exp(-gate)))).astype(BF)
    for store in stores:
        store.wait()


def retention_heads(queries, keys, values, gates, log_decay, lane, down, weight):
    count = queries.shape[0]
    positions = (lax.axis_index(EP) * count + jnp.arange(count, dtype=jnp.int32)).astype(F32)
    half = HEAD // 2
    inverse = 10000.0 ** (-jnp.arange(half, dtype=F32) / half)
    angles = positions[:, None] * jnp.concatenate([inverse, inverse])[None, :]
    cosine = jnp.cos(angles)
    sine = jnp.sin(angles) * jnp.where(jnp.arange(HEAD) < half, -1.0, 1.0)[None, :]
    flat = pltpu.HBM((count, HEAD), F32)
    base, q_decayed, pay = call(
        local_body,
        [flat, flat, onchip((PAY, HEAD), BF)],
        queries,
        keys,
        values,
        log_decay.reshape(count // BLOCK, BLOCK),
        cosine,
        sine,
        kinds="ppppvv",
        outs="hhv",
    )
    place = lax.axis_index(("ep_1", "ep_2")).reshape(1)
    near = lax.all_gather(pay, ("ep_1", "ep_2"))
    pay = call(
        quad_body,
        onchip((PAY - HEAD // 2, HEAD), BF),
        lax.axis_index("ep_2").reshape(1),
        near,
        kinds="sv",
    )
    block = (down.shape[0], down.shape[2] + weight.shape[2], HEAD)
    far = lax.all_gather(pay, ("ep_0", "ep_2"))
    return call(
        head_body,
        [shaped((count, HEAD), BF), pltpu.HBM(block, BF), pltpu.HBM(block, BF)],
        place,
        lax.axis_index("ep_0").reshape(1),
        lane.reshape(1),
        far,
        near,
        base,
        q_decayed,
        gates,
        down,
        weight,
        kinds="ssshhpphaa",
        outs="haa",
        scratch=[pltpu.VMEM((2, *block), BF), pltpu.SemaphoreType.DMA((6,))],
    )


def cut_body(far, lane, down, heads, *rest):
    peers = down.shape[1]
    outs, sems = rest[: len(far)], rest[len(far)]
    units = down.shape[2]
    copies = []
    for k, step in enumerate(far):
        at = (lane[0] + step) % peers
        copies.append(
            pltpu.make_async_copy(down.at[:, at], outs[k].at[:, 0:units], sems.at[2 * k])
        )
        copies.append(
            pltpu.make_async_copy(heads.at[:, at], outs[k].at[:, units:], sems.at[2 * k + 1])
        )
    for copy in copies:
        copy.start()
    for copy in copies:
        copy.wait()


def shifted(array, axis, far):
    peers = lax.axis_size(axis)
    return lax.ppermute(array, axis, [(k, (k + far) % peers) for k in range(peers)])


def by_peer(array, rows, peers):
    return array.reshape(rows, peers, -1, HEAD)


def exchanged_weights(down, weight, one, three, lane):
    shape = one.shape
    two = call(
        functools.partial(cut_body, (2,)),
        onchip(shape, BF),
        lane.reshape(1),
        down,
        weight,
        kinds="saa",
        scratch=[pltpu.SemaphoreType.DMA((2,))],
    )
    swapped = []
    for far, block in ((1, one), (2, two), (3, three)):
        swapped.append(shifted(block, "tp_1", far))
    return [down, weight, *swapped]


def both_halves(
    queries,
    keys,
    values,
    gates,
    log_decay,
    out_weight,
    moe_rows,
    moe_gain,
    routes,
    route_weights,
    gate_proj,
    up_proj,
    down_proj,
):
    experts = lax.axis_size(EP)
    members = lax.axis_size(TP)
    tokens = moe_rows.shape[0]
    positions = queries.shape[0]
    lane = lax.axis_index("tp_1")
    room = 2 * tokens // experts
    count = experts * room
    rows_y = lax.axis_size("tp_0")
    peers = lax.axis_size("tp_1")
    units = gate_proj.shape[2]
    tall = 2 * count + positions
    send, slots = dispatch(moe_rows, moe_gain, routes, experts, lax.axis_index(TP).reshape(1))
    down = by_peer(down_proj, rows_y, peers)
    weight = by_peer(out_weight, rows_y, peers)
    arrived = lax.all_to_all(send, EP, 0, 0, tiled=True)
    spread = call(
        spread_body,
        pltpu.HBM((members, count, HEAD), BF),
        arrived.reshape(count, HEAD),
        kinds="v",
        outs="a",
        scratch=[pltpu.SemaphoreType.DMA((members,))],
    )
    rows = lax.all_to_all(spread, TP, 0, 0, tiled=True)
    head_out, one, three = retention_heads(
        queries, keys, values, gates, log_decay, lane, down, weight
    )
    weights = exchanged_weights(down, weight, one, three, lane)
    width = gate_proj.shape[1]
    mixed = call(
        hidden_body,
        pltpu.HBM((rows_y, tall, HEAD), BF),
        rows,
        head_out,
        gate_proj,
        up_proj,
        kinds="vvaa",
        outs="a",
        scratch=[
            pltpu.VMEM((width, units), BF),
            pltpu.VMEM((width, units), BF),
            pltpu.VMEM((tall, HEAD), BF),
            pltpu.SemaphoreType.DMA((2, 2)),
            pltpu.SemaphoreType.DMA((rows_y, 5)),
        ],
    )
    got = lax.all_to_all(mixed, "tp_0", 0, 0, tiled=True)
    partial, *mixes = call(
        project_body,
        [onchip((peers, count, HEAD), BF)] + [shaped((positions, HEAD), BF)] * peers,
        lane.reshape(1),
        got,
        *weights,
        kinds="svaahhh",
        outs="vhhhh",
        scratch=[pltpu.VMEM(weights[-1].shape, BF), pltpu.SemaphoreType.DMA((2,))],
    )
    pieces = lax.all_to_all(partial, "tp_1", 0, 0, tiled=True)
    summed = call(add_body, onchip((experts, room, HEAD), BF), pieces, kinds="v")
    back = lax.all_to_all(summed, EP, 0, 0, tiled=True)
    gathered = [mixes[0]]
    for far in range(1, peers):
        gathered.append(shifted(mixes[far], "tp_1", peers - far))
    mixer_out = call(
        add_four_body, shaped((positions, HEAD), BF), *gathered, kinds="hhhh", outs="h"
    )
    columns, scales = lax.optimization_barrier((slots.T, route_weights))
    moe_out = call(
        combine_body, shaped((tokens, HEAD), BF), back, columns, scales, kinds="vvv", outs="h"
    )
    return (mixer_out, moe_out)


def solution(mesh):
    torus = Mesh(mesh.devices.reshape(8, 2, 2, 4, 4), ("ep_0", "ep_1", "ep_2", "tp_0", "tp_1"))
    return jax.shard_map(
        both_halves,
        mesh=torus,
        in_specs=(
            P(EP, TP),
            P(EP, TP),
            P(EP, TP),
            P(EP, TP),
            P(EP, TP),
            P(None, TP),
            P(EP, None),
            P(),
            P(EP, None),
            P(EP, None),
            P(EP, None, TP),
            P(EP, None, TP),
            P(EP, None, TP),
        ),
        out_specs=(P(EP, TP), P(EP, TP)),
        check_vma=False,
    )
```

```python
import functools

import jax
import jax.numpy as jnp
from jax import lax
from jax.experimental import pallas as pl
from jax.experimental.pallas import tpu as pltpu
from jax.sharding import Mesh
from jax.sharding import PartitionSpec as P

BLOCK = 128
HEAD = 128
EP = ("ep_0", "ep_1", "ep_2")
TP = ("tp_0", "tp_1")
BF = jnp.bfloat16
F32 = jnp.float32
HIGH = lax.Precision.HIGHEST
PAY = HEAD + 16
LIMIT = 12 * 1024 * 1024


def dot(a, b, dims=((1,), (0,)), precision=None):
    return lax.dot_general(a, b, (dims, ((), ())), precision=precision, preferred_element_type=F32)


def shaped(shape, dtype):
    return jax.ShapeDtypeStruct(shape, dtype)


def onchip(shape, dtype):
    return pltpu.VMEM(shape, dtype)


def call(body, out_shape, *args, kinds, outs="v", scratch=()):
    places = {
        "s": pl.BlockSpec(memory_space=pltpu.SMEM),
        "v": pl.BlockSpec(memory_space=pltpu.VMEM),
        "h": pl.BlockSpec(),
        "p": pl.BlockSpec(),
        "a": pl.BlockSpec(memory_space=pltpu.HBM),
    }
    held = [
        pltpu.with_memory_space_constraint(arg, {"v": pltpu.VMEM}.get(kind, pltpu.HBM))
        if kind in "vpa"
        else arg
        for arg, kind in zip(args, kinds, strict=True)
    ]
    single = not isinstance(out_shape, (list, tuple))
    out_specs = [places[kind] for kind in outs]
    return pl.pallas_call(
        body,
        in_specs=[places[kind] for kind in kinds],
        out_specs=out_specs[0] if single else out_specs,
        out_shape=out_shape,
        scratch_shapes=list(scratch),
        compiler_params=pltpu.CompilerParams(vmem_limit_bytes=LIMIT),
    )(*held)


def route_body(turn, routes_far, gain_far, source, send, slots, routes, gain, rows, sems, extra):
    tokens = rows.shape[0]
    experts = send.shape[0]
    room = send.shape[1]
    chunks = sems.shape[0]
    tall = tokens // chunks
    copies = [
        pltpu.make_async_copy(
            source.at[pl.ds(k * tall, tall)], rows.at[pl.ds(k * tall, tall)], sems.at[k]
        )
        for k in range(chunks)
    ]
    small = pltpu.make_async_copy(routes_far, routes, extra.at[0])
    scales = pltpu.make_async_copy(gain_far, gain, extra.at[1])
    small.start()
    for copy in copies:
        copy.start()
    scales.start()
    small.wait()
    first = routes[0:1, :]
    second = routes[1:2, :]
    expert = lax.broadcasted_iota(jnp.int32, (experts, tokens), 0)
    is_first = expert == first
    is_second = expert == second
    named = jnp.where(is_first | is_second, 1.0, 0.0).astype(BF)
    earlier = lax.broadcasted_iota(jnp.int32, (tokens, tokens), 0) < lax.broadcasted_iota(
        jnp.int32, (tokens, tokens), 1
    )
    rank = dot(named, jnp.where(earlier, 1.0, 0.0).astype(BF)).astype(jnp.int32)
    slot_a = first * room + jnp.sum(jnp.where(is_first, rank, 0), axis=0, keepdims=True)
    slot_b = second * room + jnp.sum(jnp.where(is_second, rank, 0), axis=0, keepdims=True)
    slots[0:1, :] = slot_a
    slots[1:2, :] = slot_b
    place = lax.broadcasted_iota(jnp.int32, (experts * room, tokens), 0)
    chosen = jnp.where((place == slot_a) | (place == slot_b), 1.0, 0.0).astype(BF)
    scales.wait()
    which = lax.broadcasted_iota(jnp.int32, gain.shape, 0) == turn[0]
    scale = jnp.sum(jnp.where(which, gain[...].astype(F32), 0.0), axis=0, keepdims=True)
    at = pl.multiple_of(turn[0] * HEAD, HEAD)
    parts = []
    for k, copy in enumerate(copies):
        copy.wait()
        wide = rows[k * tall : (k + 1) * tall, :].astype(F32)
        power = jnp.mean(wide * wide, axis=-1, keepdims=True)
        part = rows[k * tall : (k + 1) * tall, pl.ds(at, HEAD)].astype(F32)
        parts.append((part * lax.rsqrt(power + 1e-06) * scale).astype(BF))
    normed = jnp.concatenate(parts, axis=0)
    send[...] = dot(chosen, normed).astype(BF).reshape(experts, room, HEAD)


def dispatch(moe_rows, moe_gain, routes, experts, turn):
    tokens, width = moe_rows.shape
    room = 2 * tokens // experts
    return call(
        route_body,
        [onchip((experts, room, HEAD), BF), onchip((2, tokens), jnp.int32)],
        turn,
        routes.T,
        moe_gain.reshape(width // HEAD, HEAD),
        moe_rows,
        kinds="saaa",
        outs="vv",
        scratch=[
            pltpu.VMEM((2, tokens), jnp.int32),
            pltpu.VMEM((width // HEAD, HEAD), BF),
            pltpu.VMEM((tokens, width), BF),
            pltpu.SemaphoreType.DMA((8,)),
            pltpu.SemaphoreType.DMA((2,)),
        ],
    )


def spread_body(rows, out, sems):
    copies = [pltpu.make_async_copy(rows, out.at[k], sems.at[k]) for k in range(out.shape[0])]
    for copy in copies:
        copy.start()
    for copy in copies:
        copy.wait()


def hidden_body(rows, heads, w_gate, w_up, out, near_gate, near_up, near, sems, ends):
    parts, count, _ = rows.shape
    copied = out.shape[0]
    chunks = sems.shape[1]
    tall = w_gate.shape[1] // chunks
    copies = []
    for k in range(chunks):
        span = pl.ds(k * tall, tall)
        copies.append(
            (
                pltpu.make_async_copy(w_gate.at[0, span], near_gate.at[span], sems.at[0, k]),
                pltpu.make_async_copy(w_up.at[0, span], near_up.at[span], sems.at[1, k]),
            )
        )
    for kind in range(2):
        for pair in copies:
            pair[kind].start()
    near[2 * count :, :] = heads[...]
    per = parts // chunks
    half = count // 2
    final = []

    def product(side, kind, near_w):
        total = jnp.zeros((half, w_gate.shape[2]), F32)
        for k in range(chunks):
            if side == 0:
                copies[k][kind].wait()
            span = slice(side * half, (side + 1) * half)
            left = jnp.concatenate([rows[k * per + j, span, :] for j in range(per)], axis=1)
            total += dot(left, near_w[k * tall : (k + 1) * tall, :])
        return total

    gates = [product(side, 0, near_gate) for side in range(2)]
    for side in range(2):
        gate = gates[side]
        up = product(side, 1, near_up)
        hidden = (gate / (1.0 + jnp.exp(-gate)) * up).astype(BF)
        for part in range(2):
            at = part * count + side * half
            near[at : at + half, :] = hidden[:, part * HEAD : (part + 1) * HEAD]
            for k in range(copied):
                here = pl.ds(at, half)
                copy = pltpu.make_async_copy(
                    near.at[here], out.at[k, here], ends.at[k, 2 * side + part]
                )
                copy.start()
                final.append(copy)
        if side == 0:
            here = pl.ds(2 * count, heads.shape[0])
            for k in range(copied):
                copy = pltpu.make_async_copy(near.at[here], out.at[k, here], ends.at[k, 4])
                copy.start()
                final.append(copy)
    for copy in final:
        copy.wait()


def project_body(lane, got, down, weight, w_1, w_2, w_3, out, m_0, m_1, m_2, m_3, own, sems):
    peers = got.shape[0]
    positions = got.shape[1] // 5
    count = 2 * positions
    units = 2 * HEAD
    copies = [
        pltpu.make_async_copy(down.at[:, lane[0]], own.at[:, 0:units], sems.at[0]),
        pltpu.make_async_copy(weight.at[:, lane[0]], own.at[:, units:], sems.at[1]),
    ]
    for copy in copies:
        copy.start()
    left = [
        jnp.concatenate([got[k, 0:count, :], got[k, count : 2 * count, :]], axis=1)
        for k in range(peers)
    ]
    mixes = (m_0, m_1, m_2, m_3)
    for (one, two), steps in (((w_2, w_3), (2, 3)), ((own, w_1), (0, 1))):
        if steps[0] == 0:
            for copy in copies:
                copy.wait()
        expert = jnp.zeros((count, 2 * HEAD), F32)
        mixer = jnp.zeros((positions, 2 * HEAD), F32)
        for k in range(peers):
            both = jnp.concatenate([one[k], two[k]], axis=1)
            expert += dot(left[k], both[0:units])
            mixer += dot(got[k, 2 * count :, :], both[units:])
        for which, step in enumerate(steps):
            at = (lane[0] + peers - step) % peers
            cols = slice(which * HEAD, which * HEAD + HEAD)
            out[pl.ds(at, 1)] = expert[:, cols].astype(BF)[None]
            mixes[step][...] = mixer[:, cols].astype(BF)


def add_body(parts, out):
    total = parts[0].astype(F32)
    for k in range(1, parts.shape[0]):
        total += parts[k].astype(F32)
    out[...] = total.astype(BF).reshape(out.shape)


def add_four_body(p_0, p_1, p_2, p_3, out):
    out[...] = (
        (p_0[...].astype(F32) + p_1[...].astype(F32))
        + (p_2[...].astype(F32) + p_3[...].astype(F32))
    ).astype(BF)


def combine_body(back, slots, weights, out):
    experts, room, _ = back.shape
    rows = back[...].reshape(experts * room, HEAD)
    tokens = slots.shape[0]
    place = lax.broadcasted_iota(jnp.int32, (tokens, experts * room), 1)
    total = jnp.zeros((tokens, HEAD), F32)
    for k in range(2):
        chosen = jnp.where(place == slots[:, k : k + 1], 1.0, 0.0).astype(BF)
        total += dot(chosen, rows) * weights[:, k : k + 1]
    out[...] = total.astype(BF)


def local_body(q, k, v, decay, cosine, sine, base, q_decayed, pay):
    count = q.shape[0]
    blocks = count // BLOCK
    cos = cosine[...]
    sin = sine[...]
    rows = lax.broadcasted_iota(jnp.int32, (BLOCK, BLOCK), 0)
    cols = lax.broadcasted_iota(jnp.int32, (BLOCK, BLOCK), 1)
    causal = rows >= cols
    upper = jnp.where(rows <= cols, 1.0, 0.0)
    lower = jnp.where(causal, 1.0, 0.0)

    def turned(x, factor):
        wide = x.astype(F32)
        swapped = pltpu.roll(wide, HEAD // 2, 1)
        return ((wide * cos + swapped * sin) * factor).astype(BF)

    q_all = turned(q[...], 1.0)
    k_all = turned(k[...], HEAD ** (-0.5))
    carried = jnp.zeros((HEAD, HEAD), F32)
    leading = jnp.zeros((1, HEAD), F32)
    for n in range(blocks):
        span = slice(n * BLOCK, n * BLOCK + BLOCK)
        q_b, k_b, v_b = q_all[span], k_all[span], v[span, :]
        here = jnp.broadcast_to(decay[n : n + 1, :], (BLOCK, BLOCK))
        cum_i = dot(lower, here, ((1,), (1,)), HIGH)
        cum_j = dot(here, upper, precision=HIGH)
        weights = jnp.where(causal, jnp.exp(jnp.where(causal, cum_i - cum_j, 0.0)), 0.0)
        scores = dot(q_b, k_b, ((1,), (1,)))
        inside = dot((scores * weights).astype(BF), v_b)
        q_f = q_b.astype(F32)
        q_d = q_f * jnp.exp(cum_i)
        if n:
            inside += dot(q_d, carried, precision=HIGH)
        base[span, :] = inside
        q_decayed[span, :] = q_f * jnp.exp(cum_i + leading)
        ending = cum_i[BLOCK - 1 : BLOCK, :]
        k_scaled = k_b.astype(F32) * jnp.exp(ending - cum_i)
        update = dot(k_scaled, v_b.astype(F32), ((0,), (0,)), HIGH)
        carried = jnp.exp(ending) * carried + update
        leading = leading + ending
    packed(pay, carried, leading)


def packed(pay, state, total):
    pay[0 : state.shape[0], :] = state.astype(BF)
    high = total.astype(BF)
    rest = total - high.astype(F32)
    middle = rest.astype(BF)
    low = (rest - middle.astype(F32)).astype(BF)
    row = lax.broadcasted_iota(jnp.int32, (16, HEAD), 0)
    three = jnp.where(
        row == 0,
        high.astype(F32),
        jnp.where(row == 1, middle.astype(F32), jnp.where(row == 2, low.astype(F32), 0.0)),
    )
    pay[state.shape[0] :, :] = three.astype(BF)


def unpacked(pay):
    rows = pay.shape[0] - 16
    tail = pay[rows:, :].astype(F32)
    return pay[0:rows, :].astype(F32), tail[0:1] + tail[1:2] + tail[2:3]


def quad_body(core, near, pay):
    state, decay = unpacked(near.at[0])
    for k in range(1, near.shape[0]):
        later, later_decay = unpacked(near.at[k])
        state = later + jnp.exp(later_decay) * state
        decay = decay + later_decay
    half = HEAD // 2
    mine = jnp.where(core[0] == 0, state[0:half], state[half:])
    packed(pay, mine, decay)


def head_body(
    place, group, lane, far, near, base, q_decayed, gates, down, weight, out, b_1, b_3, here, sems
):
    peers = down.shape[1]
    units = down.shape[2]
    loads, stores = [], []
    for k, (step, block) in enumerate(((1, b_1), (3, b_3))):
        at = (lane[0] + step) % peers
        loads.append(
            (
                pltpu.make_async_copy(down.at[:, at], here.at[k, :, 0:units], sems.at[3 * k]),
                pltpu.make_async_copy(weight.at[:, at], here.at[k, :, units:], sems.at[3 * k + 1]),
            )
        )
        stores.append(pltpu.make_async_copy(here.at[k], block, sems.at[3 * k + 2]))
    for one, two in loads:
        one.start()
        two.start()
    entering = jnp.zeros((HEAD, HEAD), F32)
    for k in range(far.shape[0] // 2):
        upper, decay = unpacked(far.at[2 * k])
        lower, _ = unpacked(far.at[2 * k + 1])
        state = jnp.concatenate([upper, lower], axis=0)
        entering = jnp.where(k < group[0], jnp.exp(decay) * entering + state, entering)
    for k in range(near.shape[0] - 1):
        state, decay = unpacked(near.at[k])
        entering = jnp.where(k < place[0], jnp.exp(decay) * entering + state, entering)
    for (one, two), store in zip(loads, stores, strict=True):
        one.wait()
        two.wait()
        store.start()
    retained = base[...] + dot(q_decayed[...], entering, precision=HIGH)
    power = jnp.mean(retained * retained, axis=-1, keepdims=True)
    gate = gates[...].astype(F32)
    out[...] = (retained * lax.rsqrt(power + 1e-05) * (gate / (1.0 + jnp.exp(-gate)))).astype(BF)
    for store in stores:
        store.wait()


def retention_heads(queries, keys, values, gates, log_decay, lane, down, weight):
    count = queries.shape[0]
    positions = (lax.axis_index(EP) * count + jnp.arange(count, dtype=jnp.int32)).astype(F32)
    half = HEAD // 2
    inverse = 10000.0 ** (-jnp.arange(half, dtype=F32) / half)
    angles = positions[:, None] * jnp.concatenate([inverse, inverse])[None, :]
    cosine = jnp.cos(angles)
    sine = jnp.sin(angles) * jnp.where(jnp.arange(HEAD) < half, -1.0, 1.0)[None, :]
    flat = pltpu.HBM((count, HEAD), F32)
    base, q_decayed, pay = call(
        local_body,
        [flat, flat, onchip((PAY, HEAD), BF)],
        queries,
        keys,
        values,
        log_decay.reshape(count // BLOCK, BLOCK),
        cosine,
        sine,
        kinds="ppppvv",
        outs="hhv",
    )
    place = lax.axis_index(("ep_1", "ep_2")).reshape(1)
    near = lax.all_gather(pay, ("ep_1", "ep_2"))
    pay = call(
        quad_body,
        onchip((PAY - HEAD // 2, HEAD), BF),
        lax.axis_index("ep_2").reshape(1),
        near,
        kinds="sv",
    )
    block = (down.shape[0], down.shape[2] + weight.shape[2], HEAD)
    far = lax.all_gather(pay, ("ep_0", "ep_2"))
    return call(
        head_body,
        [shaped((count, HEAD), BF), pltpu.HBM(block, BF), pltpu.HBM(block, BF)],
        place,
        lax.axis_index("ep_0").reshape(1),
        lane.reshape(1),
        far,
        near,
        base,
        q_decayed,
        gates,
        down,
        weight,
        kinds="ssshhpphaa",
        outs="haa",
        scratch=[pltpu.VMEM((2, *block), BF), pltpu.SemaphoreType.DMA((6,))],
    )


def cut_body(far, lane, down, heads, *rest):
    peers = down.shape[1]
    outs, sems = rest[: len(far)], rest[len(far)]
    units = down.shape[2]
    copies = []
    for k, step in enumerate(far):
        at = (lane[0] + step) % peers
        copies.append(
            pltpu.make_async_copy(down.at[:, at], outs[k].at[:, 0:units], sems.at[2 * k])
        )
        copies.append(
            pltpu.make_async_copy(heads.at[:, at], outs[k].at[:, units:], sems.at[2 * k + 1])
        )
    for copy in copies:
        copy.start()
    for copy in copies:
        copy.wait()


def shifted(array, axis, far):
    peers = lax.axis_size(axis)
    return lax.ppermute(array, axis, [(k, (k + far) % peers) for k in range(peers)])


def by_peer(array, rows, peers):
    return array.reshape(rows, peers, -1, HEAD)


def exchanged_weights(down, weight, one, three, lane):
    shape = one.shape
    two = call(
        functools.partial(cut_body, (2,)),
        onchip(shape, BF),
        lane.reshape(1),
        down,
        weight,
        kinds="saa",
        scratch=[pltpu.SemaphoreType.DMA((2,))],
    )
    swapped = []
    for far, block in ((1, one), (2, two), (3, three)):
        swapped.append(shifted(block, "tp_1", far))
    return [down, weight, *swapped]


def both_halves(
    queries,
    keys,
    values,
    gates,
    log_decay,
    out_weight,
    moe_rows,
    moe_gain,
    routes,
    route_weights,
    gate_proj,
    up_proj,
    down_proj,
):
    experts = lax.axis_size(EP)
    members = lax.axis_size(TP)
    tokens = moe_rows.shape[0]
    positions = queries.shape[0]
    lane = lax.axis_index("tp_1")
    room = 2 * tokens // experts
    count = experts * room
    rows_y = lax.axis_size("tp_0")
    peers = lax.axis_size("tp_1")
    units = gate_proj.shape[2]
    tall = 2 * count + positions
    send, slots = dispatch(moe_rows, moe_gain, routes, experts, lax.axis_index(TP).reshape(1))
    down = by_peer(down_proj, rows_y, peers)
    weight = by_peer(out_weight, rows_y, peers)
    arrived = lax.all_to_all(send, EP, 0, 0, tiled=True)
    spread = call(
        spread_body,
        pltpu.HBM((members, count, HEAD), BF),
        arrived.reshape(count, HEAD),
        kinds="v",
        outs="a",
        scratch=[pltpu.SemaphoreType.DMA((members,))],
    )
    rows = lax.all_to_all(spread, TP, 0, 0, tiled=True)
    head_out, one, three = retention_heads(
        queries, keys, values, gates, log_decay, lane, down, weight
    )
    weights = exchanged_weights(down, weight, one, three, lane)
    width = gate_proj.shape[1]
    mixed = call(
        hidden_body,
        pltpu.HBM((rows_y, tall, HEAD), BF),
        rows,
        head_out,
        gate_proj,
        up_proj,
        kinds="vvaa",
        outs="a",
        scratch=[
            pltpu.VMEM((width, units), BF),
            pltpu.VMEM((width, units), BF),
            pltpu.VMEM((tall, HEAD), BF),
            pltpu.SemaphoreType.DMA((2, 2)),
            pltpu.SemaphoreType.DMA((rows_y, 5)),
        ],
    )
    got = lax.all_to_all(mixed, "tp_0", 0, 0, tiled=True)
    partial, *mixes = call(
        project_body,
        [onchip((peers, count, HEAD), BF)] + [shaped((positions, HEAD), BF)] * peers,
        lane.reshape(1),
        got,
        *weights,
        kinds="svaahhh",
        outs="vhhhh",
        scratch=[pltpu.VMEM(weights[-1].shape, BF), pltpu.SemaphoreType.DMA((2,))],
    )
    pieces = lax.all_to_all(partial, "tp_1", 0, 0, tiled=True)
    summed = call(add_body, onchip((experts, room, HEAD), BF), pieces, kinds="v")
    back = lax.all_to_all(summed, EP, 0, 0, tiled=True)
    gathered = [mixes[0]]
    for far in range(1, peers):
        gathered.append(shifted(mixes[far], "tp_1", peers - far))
    mixer_out = call(
        add_four_body, shaped((positions, HEAD), BF), *gathered, kinds="hhhh", outs="h"
    )
    columns, scales = lax.optimization_barrier((slots.T, route_weights))
    moe_out = call(
        combine_body, shaped((tokens, HEAD), BF), back, columns, scales, kinds="vvv", outs="h"
    )
    return (mixer_out, moe_out)


def solution(mesh):
    torus = Mesh(mesh.devices.reshape(8, 2, 2, 4, 4), ("ep_0", "ep_1", "ep_2", "tp_0", "tp_1"))
    return jax.shard_map(
        both_halves,
        mesh=torus,
        in_specs=(
            P(EP, TP),
            P(EP, TP),
            P(EP, TP),
            P(EP, TP),
            P(EP, TP),
            P(None, TP),
            P(EP, None),
            P(),
            P(EP, None),
            P(EP, None),
            P(EP, None, TP),
            P(EP, None, TP),
            P(EP, None, TP),
        ),
        out_specs=(P(EP, TP), P(EP, TP)),
        check_vma=False,
    )
```
